128 devices in a mesh: sp: 16 (over z, x), tp: 8 (over y, core).
Axes of the slice: x: 4, y: 4, z: 4, core: 2. Of those that a mesh axis runs over, the one named last changes fastest.
Arguments:
- out_gate: bfloat16 [16384, 1536], P('sp', 'tp'), may hold values from -6 to 6
- in_gate: bfloat16 [16384, 1536], P('sp', 'tp'), may hold values from -6 to 6
- conv_values: bfloat16 [16384, 1536], P('sp', 'tp'), may hold values from -6 to 6
- conv_taps: float32 [3, 1536], P(None, 'tp'), may hold values from -3 to 3
- mix_gain: float32 [1536], replicated, may hold values from 0.1 to 1.9
- out_proj: bfloat16 [1536, 2048], replicated, may hold values from -0.15625 to 0.15625
- residual: bfloat16 [16384, 2048], P(('sp', 'tp')), may hold values from -6 to 6
- ffn_gain: float32 [2048], replicated, may hold values from 0.1 to 1.9
- routes: int32 [16384, 6], P(('sp', 'tp')), may hold values from 0 to 127, all different within a row; in each aligned block of 128 rows (0 to 127, 128 to 255, ...) at most 8 rows name the same one
- route_weights: float32 [16384, 6], P(('sp', 'tp')), may hold values from 0.05 to 1
- shared_gate: bfloat16 [2048, 512], replicated, may hold values from -0.125 to 0.125
- shared_up: bfloat16 [2048, 512], replicated, may hold values from -0.125 to 0.125
- shared_down: bfloat16 [512, 2048], replicated, may hold values from -0.25 to 0.25
- expert_gate: bfloat16 [128, 2048, 512], P(('sp', 'tp')), may hold values from -0.125 to 0.125
- expert_up: bfloat16 [128, 2048, 512], P(('sp', 'tp')), may hold values from -0.125 to 0.125
- expert_down: bfloat16 [128, 512, 2048], P(('sp', 'tp')), may hold values from -0.25 to 0.25
Outputs:
- layer_out: bfloat16 [16384, 2048], P(('sp', 'tp'))
The draws below stay inside these ranges and needn't reach their ends.
Inputs may be any that keep to these rules, and one draw needn't show every extreme that they name: `routes`: each row names 6 different experts. Within the rows of one device (aligned blocks of 128 rows) no expert is named more than 8 times, a bound that some block reaches.
All inputs are finite; a program needn't handle non-finite values.
Results may differ from the reference program's by a relative error of at most 0.0065.
Values may be sent and summed in bfloat16 or wider, within the bound.
A program may use at most 128 MiB of HBM per device.

```python
import math
import jax
import jax.numpy as jnp
import numpy as np
from jax import lax

D = 2048
DC = 1536
KERNEL = 3
FF_E = 512
FS = 512
TOP = 6
ROWS_DEV = 128
TOKENS = 16384
EXPERTS = 128
CAP = 8
N_SP = 16
N_TP = 8


def levels(key, shape, shards, smallest, largest):
    level = 1.0
    for axis_at, parts in shards:
        steps = jax.random.uniform(jax.random.fold_in(jax.random.fold_in(key, 6), axis_at), (parts,), jnp.float32, smallest / len(shards), largest / len(shards))
        level = level * jnp.repeat(jnp.exp(steps), shape[axis_at] // parts).reshape((-1,) + (1,) * (len(shape) - 1 - axis_at))
    return level


def deal_out(stream_key, own, number, rows, number_of, top, limit, slope):
    order = jax.random.permutation(stream_key, number_of)
    packed, common = portions_of(number_of, rows * top, limit, slope, True), portions_of(number_of, rows * top, limit, slope, False)
    places = jnp.arange(number_of)

    def named(sizes, offset_by):
        used = int((sizes > 0).sum())
        fixed = max(1, used // 4)
        passed = fixed + (places - fixed + offset_by * (used - fixed)) % max(1, number_of - fixed)
        return jnp.zeros((number_of,), jnp.int32).at[order[jnp.where(places < fixed, places, passed)]].set(jnp.asarray(sizes, jnp.int32))

    sizes = jnp.where(number % 4 == 0, named(packed, number // 4), named(common, number - number // 4 - 1))
    mixed = jax.random.permutation(jax.random.fold_in(own, 3), number_of)
    source_of, taker = mixed[0:number_of // 2 * 2:2], mixed[1:number_of // 2 * 2:2]
    margin = jnp.minimum(sizes[source_of] - 1, limit - sizes[taker]) // 2
    margin = jnp.where((source_of == order[0]) | (taker == order[0]) | (sizes[taker] == 0), 0, jnp.maximum(margin, 0))
    passed = jax.random.randint(jax.random.fold_in(own, 4), (number_of // 2,), 0, 1 << 20) % (margin + 1)
    sizes = sizes.at[source_of].add(-passed).at[taker].add(passed)
    labels = jnp.searchsorted(jnp.cumsum(sizes), jnp.arange(rows * top), side="right").astype(jnp.int32)
    listing = labels.reshape(top, rows).T
    listing = listing[jax.random.permutation(jax.random.fold_in(own, 1), rows)]
    offset_by = jax.random.randint(jax.random.fold_in(own, 2), (rows, 1), 0, top)
    return jnp.take_along_axis(listing, (jnp.arange(top)[None, :] + offset_by) % top, axis=1)


def portions_of(count, total, reach, slope, full):
    portions = [(1 << 20) // math.isqrt(rank ** slope) + 1 for rank in range(1, count + 1)]
    largest = reach if full else min(reach, max(-(-total // count), total * portions[0] // sum(portions)))
    least = 1 if total - largest >= count - 1 else 0
    given, surplus = [largest] + [least] * (count - 1), total - largest - least * (count - 1)
    while surplus > 0:
        movable = [i for i in range(1, count) if given[i] < largest] or [i for i in range(1, count) if given[i] < reach]
        whole, remaining = sum([portions[i] for i in movable]), surplus
        for i in movable:
            addition = min(reach - given[i], max(1, remaining * portions[i] // whole), surplus)
            given[i] = given[i] + addition
            surplus = surplus - addition
    return np.array(given)


def gaussian(own_key, shape, deviation, limit, split=(), kind=jnp.bfloat16):
    values = jax.random.normal(own_key, shape, jnp.float32) * deviation
    if len(split) > 0:
        values = levels(own_key, shape, split, -0.22, 0.18) * values
    return jnp.clip(values, min=-limit, max=limit).astype(kind)


def setup_inputs(seed: int = 0) -> dict:
    splits = jax.random.split(jax.random.key(seed), 17)
    out_gate = gaussian(splits[0], (TOKENS, DC), 1.0, 6.0, ((0, 16), (1, 8)))
    in_gate = gaussian(splits[1], (TOKENS, DC), 1.0, 6.0, ((0, 16), (1, 8)))
    conv_values = gaussian(splits[2], (TOKENS, DC), 1.0, 6.0, ((0, 16), (1, 8)))
    conv_taps = gaussian(splits[3], (KERNEL, DC), 0.6, 3.0, ((1, 8),), jnp.float32)
    mix_gain = jnp.clip(1.0 + 0.18 * jax.random.normal(splits[4], (DC,), jnp.float32), 0.1, 1.9)
    out_proj = gaussian(splits[5], (DC, D), DC ** -0.5, 0.15625)
    residual = gaussian(splits[6], (TOKENS, D), 1.0, 6.0, ((0, 128),))
    ffn_gain = jnp.clip(1.0 + 0.18 * jax.random.normal(splits[7], (D,), jnp.float32), 0.1, 1.9)
    routes_keys = jax.random.split(jax.random.fold_in(splits[8], 1), TOKENS // ROWS_DEV)
    routes_turns = jax.random.permutation(jax.random.fold_in(splits[8], 3), TOKENS // ROWS_DEV)
    routes = jax.vmap(lambda own, number: deal_out(jax.random.fold_in(splits[8], 2), own, number, ROWS_DEV, EXPERTS, TOP, CAP, 2))(routes_keys, routes_turns).reshape((TOKENS, TOP))
    route_weights = jnp.clip(jnp.exp(math.log(1.0) - 2.9957323 * jax.random.uniform(splits[9], (TOKENS, TOP), jnp.float32) ** levels(splits[9], (TOKENS, TOP), ((0, 128),), -0.2, 0.2)), 0.05, 1.0)
    shared_gate = gaussian(splits[10], (D, FS), D ** -0.5, 0.125)
    shared_up = gaussian(splits[11], (D, FS), D ** -0.5, 0.125)
    shared_down = gaussian(splits[12], (FS, D), FS ** -0.5, 0.25)
    expert_gate = gaussian(splits[13], (EXPERTS, D, FF_E), D ** -0.5, 0.125, ((0, 128),))
    expert_up = gaussian(splits[14], (EXPERTS, D, FF_E), D ** -0.5, 0.125, ((0, 128),))
    expert_down = gaussian(splits[15], (EXPERTS, FF_E, D), FF_E ** -0.5, 0.25, ((0, 128),))
    return dict(out_gate=out_gate, in_gate=in_gate, conv_values=conv_values, conv_taps=conv_taps, mix_gain=mix_gain, out_proj=out_proj, residual=residual, ffn_gain=ffn_gain, routes=routes, route_weights=route_weights, shared_gate=shared_gate, shared_up=shared_up, shared_down=shared_down, expert_gate=expert_gate, expert_up=expert_up, expert_down=expert_down)


def project_norm(conv_out, mix_gain, out_proj):
    values = conv_out.astype(jnp.float32)
    inverse = lax.rsqrt(lax.optimization_barrier(jnp.mean(values * values, axis=-1)) + 1e-06)
    scaled = (values * mix_gain).astype(jnp.bfloat16)
    return jnp.dot(scaled, out_proj, preferred_element_type=jnp.float32) * inverse[:, None]

def ffn_input(stream, ffn_gain):
    inverse = lax.rsqrt(lax.optimization_barrier(jnp.mean(stream * stream, axis=-1, keepdims=True)) + 1e-06)
    return (stream * inverse * ffn_gain).astype(jnp.bfloat16)

def swiglu_hidden(row_block, weight_gate, weight_up):
    gate_part = jnp.dot(row_block, weight_gate, preferred_element_type=jnp.float32)
    up_part = jnp.dot(row_block, weight_up, preferred_element_type=jnp.float32)
    return (jax.nn.silu(gate_part) * up_part).astype(jnp.bfloat16)

def reference(out_gate, in_gate, conv_values, conv_taps, mix_gain, out_proj, residual, ffn_gain, routes, route_weights, shared_gate, shared_up, shared_down, expert_gate, expert_up, expert_down):
    mixed_in = in_gate.astype(jnp.float32) * conv_values.astype(jnp.float32)
    taps_count = conv_taps.shape[0]
    length = mixed_in.shape[0]
    extended = jnp.concatenate([jnp.zeros((taps_count - 1, mixed_in.shape[1]), jnp.float32), mixed_in], axis=0)
    filtered = conv_taps[0] * extended[0:length]
    for offset in range(1, taps_count):
        filtered = filtered + conv_taps[offset] * extended[offset:offset + length]
    conv_out = (out_gate.astype(jnp.float32) * filtered).astype(jnp.bfloat16)
    stream = residual.astype(jnp.float32) + project_norm(conv_out, mix_gain, out_proj)
    normed = ffn_input(stream, ffn_gain)
    shared_result = jnp.dot(swiglu_hidden(normed, shared_gate, shared_up), shared_down, preferred_element_type=jnp.float32)
    top_count = routes.shape[1]
    token_count = routes.shape[0]
    model_width = normed.shape[1]
    flat_ids = routes.reshape(-1).astype(jnp.int32)
    gate_values = route_weights / lax.optimization_barrier(jnp.sum(route_weights, axis=1, keepdims=True)) * 2.5
    flat_gates = gate_values.reshape(-1)
    sort_order = jnp.argsort(flat_ids, stable=True).astype(jnp.int32)
    sorted_ids = flat_ids[sort_order]
    counts = jnp.bincount(flat_ids, length=EXPERTS).astype(jnp.int32)
    starts = (jnp.cumsum(counts) - counts).astype(jnp.int32)
    slot_rank = jnp.arange(flat_ids.shape[0], dtype=jnp.int32) - starts[sorted_ids]
    most_rows = N_SP * N_TP * CAP
    slot_index = (sorted_ids * most_rows + slot_rank).astype(jnp.int32)
    row_of = (sort_order // top_count).astype(jnp.int32)
    slot_rows = jnp.full((EXPERTS * most_rows,), token_count, jnp.int32).at[slot_index].set(row_of)
    slot_gates = jnp.zeros((EXPERTS * most_rows,), jnp.float32).at[slot_index].set(flat_gates[sort_order])
    padded = jnp.concatenate([normed, jnp.zeros((1, model_width), jnp.bfloat16)], axis=0)

    def add_expert(running, inputs):
        row_index, gate_slots, weight_gate, weight_up, weight_down = inputs
        picked = padded[row_index]
        hidden = swiglu_hidden(picked, weight_gate, weight_up)
        result = jnp.dot(hidden, weight_down, preferred_element_type=jnp.float32).astype(jnp.bfloat16)
        return (running.at[row_index].add(result.astype(jnp.float32) * gate_slots[:, None]), None)
    running = jnp.zeros((token_count + 1, model_width), jnp.float32)
    running, _ = lax.scan(add_expert, running, (slot_rows.reshape(EXPERTS, most_rows), slot_gates.reshape(EXPERTS, most_rows), expert_gate, expert_up, expert_down))
    routed = running[:token_count]
    return (stream + shared_result + routed).astype(jnp.bfloat16)
```

```python
import jax
import jax.numpy as jnp
from jax import lax
from jax.sharding import PartitionSpec as P


def from_behind(block, axis, distance):
    devices = range(lax.axis_size(axis))
    route = [(i - distance, i) for i in devices if i - distance in devices]
    return lax.ppermute(block, axis, route)


def project_norm(conv_out, mix_gain, out_proj):
    values = conv_out.astype(jnp.float32)
    inverse = lax.rsqrt(jnp.mean(values * values, axis=-1) + 1e-06)
    scaled = (values * mix_gain).astype(jnp.bfloat16)
    return jnp.dot(scaled, out_proj, preferred_element_type=jnp.float32) * inverse[:, None]


def swiglu_hidden(row_block, weight_gate, weight_up):
    gate_part = jnp.dot(row_block, weight_gate, preferred_element_type=jnp.float32)
    up_part = jnp.dot(row_block, weight_up, preferred_element_type=jnp.float32)
    return (jax.nn.silu(gate_part) * up_part).astype(jnp.bfloat16)


def body(
    out_gate,
    in_gate,
    conv_values,
    conv_taps,
    mix_gain,
    out_proj,
    residual,
    ffn_gain,
    routes,
    route_weights,
    shared_gate,
    shared_up,
    shared_down,
    expert_gate,
    expert_up,
    expert_down,
):
    mixed_in = in_gate.astype(jnp.float32) * conv_values.astype(jnp.float32)
    taps_count = conv_taps.shape[0]
    length = mixed_in.shape[0]
    earlier = from_behind(mixed_in[length - (taps_count - 1) :], "sp", 1)
    extended = jnp.concatenate([earlier, mixed_in], axis=0)
    filtered = conv_taps[0] * extended[0:length]
    for offset in range(1, taps_count):
        filtered = filtered + conv_taps[offset] * extended[offset : offset + length]
    conv_out = (out_gate.astype(jnp.float32) * filtered).astype(jnp.bfloat16)
    row_count = length // lax.axis_size("tp")
    token_rows = lax.all_to_all(conv_out, "tp", split_axis=0, concat_axis=1, tiled=True)
    mix_result = project_norm(token_rows, mix_gain, out_proj)
    stream = residual.astype(jnp.float32) + mix_result
    norm_inverse = lax.rsqrt(jnp.mean(stream * stream, axis=-1, keepdims=True) + 1e-06)
    normed = (stream * norm_inverse * ffn_gain).astype(jnp.bfloat16)
    shared_result = jnp.dot(
        swiglu_hidden(normed, shared_gate, shared_up),
        shared_down,
        preferred_element_type=jnp.float32,
    )
    model_width = normed.shape[1]
    sp_count = lax.axis_size("sp")
    tp_count = lax.axis_size("tp")
    experts_total = sp_count * tp_count
    top_count = routes.shape[1]
    capacity = max(2, 4 * row_count * top_count // (3 * experts_total))
    expert_ids = jnp.arange(experts_total, dtype=jnp.int32)
    named = routes.T[:, None, :] == expert_ids[None, :, None]
    mask = jnp.sum(named.astype(jnp.float32), axis=0)
    earlier_rows = jnp.triu(jnp.ones((row_count, row_count), jnp.bfloat16), 1)
    rank = jnp.dot(mask.astype(jnp.bfloat16), earlier_rows, preferred_element_type=jnp.float32)
    gate_values = route_weights / jnp.sum(route_weights, axis=1, keepdims=True) * 2.5
    gates = jnp.sum(jnp.where(named, gate_values.T[:, None, :], 0.0), axis=0)
    slot_ranks = jnp.arange(capacity, dtype=jnp.float32)[None, :, None]
    chosen = (rank[:, None, :] == slot_ranks) & (mask[:, None, :] > 0)
    select = chosen.astype(jnp.bfloat16).reshape(experts_total * capacity, row_count)
    weight = jnp.where(chosen, gates[:, None, :], 0.0).reshape(experts_total * capacity, row_count)
    weight_high = weight.astype(jnp.bfloat16)
    weight_low = (weight - weight_high.astype(jnp.float32)).astype(jnp.bfloat16)
    outgoing = jnp.dot(select, normed, preferred_element_type=jnp.float32).astype(jnp.bfloat16)
    outgoing = outgoing.reshape(experts_total, capacity, model_width)
    arrived = lax.all_to_all(outgoing, ("sp", "tp"), split_axis=0, concat_axis=0, tiled=True)
    leading = arrived.shape[:-1]
    hidden = swiglu_hidden(arrived.reshape(-1, model_width), expert_gate[0], expert_up[0])
    result = jnp.dot(hidden, expert_down[0], preferred_element_type=jnp.float32).astype(
        jnp.bfloat16
    )
    returned_rows = lax.all_to_all(
        result.reshape(leading + (model_width,)),
        ("sp", "tp"),
        split_axis=0,
        concat_axis=0,
        tiled=True,
    )
    flat_returned = returned_rows.reshape(experts_total * capacity, model_width)
    transposed = (((0,), (0,)), ((), ()))
    routed = lax.dot_general(
        weight_high, flat_returned, transposed, preferred_element_type=jnp.float32
    ) + lax.dot_general(
        weight_low, flat_returned, transposed, preferred_element_type=jnp.float32
    )
    return (stream + shared_result + routed).astype(jnp.bfloat16)


def solution(mesh):
    in_specs = (
        P("sp", "tp"),
        P("sp", "tp"),
        P("sp", "tp"),
        P(None, "tp"),
        P(),
        P(),
        P(("sp", "tp"), None),
        P(),
        P(("sp", "tp"), None),
        P(("sp", "tp"), None),
        P(),
        P(),
        P(),
        P(("sp", "tp"), None, None),
        P(("sp", "tp"), None, None),
        P(("sp", "tp"), None, None),
    )
    out_specs = P(("sp", "tp"), None)
    return jax.shard_map(body, mesh=mesh, in_specs=in_specs, out_specs=out_specs, check_vma=False)
```

```python
import jax
import jax.numpy as jnp
import numpy as np
from jax import lax
from jax.experimental import pallas as pl
from jax.experimental.pallas import tpu as pltpu
from jax.sharding import PartitionSpec as P


COLORS = (("z", "x", "y", 0, 640), ("x", "y", "z", 640, 640), ("y", "z", "x", 1280, 768))
AXES = ("z", "x", "y")
RING = 4
CORES = 2
SLOTS = 8
MESH = pl.DeviceIdType.MESH
PAIRS = tuple((g, h) for g in range(RING) for h in range(CORES) if (g, h) != (0, 0))
NEAR_FIRST = (1, 3, 2)


def expansion_table(experts_total):
    slot = np.arange(experts_total * SLOTS)
    ids = []
    for first, second, third, _, _ in COLORS:
        digits = {
            first: slot // (RING * RING * CORES * SLOTS) % RING,
            second: slot // (RING * CORES * SLOTS) % RING,
            third: slot // (CORES * SLOTS) % RING,
        }
        core = slot // SLOTS % CORES
        ids.append(((digits["z"] * RING + digits["x"]) * RING + digits["y"]) * CORES + core)
    return np.concatenate(ids)


def slot_tables(routes, route_weights, experts_total):
    row_count = routes.shape[0]
    expert_ids = jnp.arange(experts_total, dtype=jnp.int32)
    gate_values = route_weights / jnp.sum(route_weights, axis=1, keepdims=True) * 2.5
    named = routes[:, :, None] == expert_ids[None, None, :]
    mask = jnp.sum(named.astype(jnp.float32), axis=1)
    gates = jnp.sum(jnp.where(named, gate_values[:, :, None], 0.0), axis=1)
    earlier = jnp.tril(jnp.ones((row_count, row_count), jnp.bfloat16), -1)
    rank = jnp.dot(earlier, mask.astype(jnp.bfloat16), preferred_element_type=jnp.float32)
    ranks = jnp.arange(SLOTS, dtype=jnp.float32)[:, None, None]
    chosen = (rank[None] == ranks) & (mask[None] > 0)
    numbers = jnp.arange(1, row_count + 1, dtype=jnp.float32)[None, :, None]
    token = jnp.sum(jnp.where(chosen, numbers, 0.0), axis=1)
    gate = jnp.sum(jnp.where(chosen, gates[None], 0.0), axis=1)
    high = gate.astype(jnp.bfloat16)
    low = (gate - high.astype(jnp.float32)).astype(jnp.bfloat16)
    stacked = jnp.concatenate([token.astype(jnp.bfloat16), high, low], axis=0)
    ids = jnp.asarray(expansion_table(experts_total), jnp.int32)
    expand = (expert_ids[:, None] == ids[None, :]).astype(jnp.bfloat16)
    spread = jnp.dot(stacked, expand, preferred_element_type=jnp.float32)
    slot_rank = jnp.arange(ids.shape[0], dtype=jnp.int32) % SLOTS
    keep = jnp.arange(SLOTS, dtype=jnp.int32)[:, None] == slot_rank[None, :]
    rows = jnp.sum(jnp.where(keep[None], spread.reshape(3, SLOTS, -1), 0.0), axis=1)
    rows = rows.reshape(3, len(COLORS), RING, -1).transpose(1, 2, 0, 3)
    return jnp.pad(rows, ((0, 0), (0, 0), (0, SLOTS - 3), (0, 0)))


def moe_kernel(
    normed, tables, base, w_gate, w_up, w_down, out,
    v_gate, v_up, v_down, seen_tab, arrived, result, total, own_part,
    ag0, ag1, ag2, pick0, pick1, pick2, mid0, mid1, mid2,
    back0, back1, back2, slots0, slots1, slots2, part0, part1, part2, got0, got1, got2,
    w_sem, tab_s, tab_r, ag_s, ag_r, p2_s, p2_r, p3_s, p3_r, r1_s, r1_r, r2_s, r2_r, r3_s, r3_r,
):
    ag, pick, mid = (ag0, ag1, ag2), (pick0, pick1, pick2), (mid0, mid1, mid2)
    back, slots = (back0, back1, back2), (slots0, slots1, slots2)
    part, got = (part0, part1, part2), (got0, got1, got2)
    sp, tp = lax.axis_index("sp"), lax.axis_index("tp")
    at = {"z": sp // RING, "x": sp % RING, "y": tp // CORES}
    core = tp % CORES

    def device(core_step=0, **steps):
        p = {k: (at[k] + steps.get(k, 0)) % RING for k in AXES}
        return (p["z"] * RING + p["x"], p["y"] * CORES + (core + core_step) % CORES)

    def send(src, dst, s, r, target):
        copy = pltpu.make_async_remote_copy(
            src_ref=src, dst_ref=dst, send_sem=s, recv_sem=r, device_id=target, device_id_type=MESH
        )
        copy.start()
        return copy

    def lead(q, i, d):
        return (d, i) if q == 2 else (i, d)

    def piece(ref, q, g, h):
        c0, w = COLORS[q][3:]
        cols = pl.ds(c0, w)
        if q == 0:
            return ref.at[:, :, g, h, :, cols]
        if q == 1:
            return ref.at[g, :, :, h, :, cols]
        return ref.at[:, g, :, h, :, cols]

    loads = [
        pltpu.make_async_copy(src, dst, w_sem.at[n])
        for n, (src, dst) in enumerate(((w_gate, v_gate), (w_up, v_up), (w_down, v_down)))
    ]
    for load in loads:
        load.start()

    barrier = pltpu.get_barrier_semaphore()
    peers = [device(1)] + [
        device(h, **{axis: g}) for axis in AXES for g in range(1, RING) for h in range(CORES)
    ]
    for peer in peers:
        pl.semaphore_signal(barrier, inc=1, device_id=peer, device_id_type=MESH)
    pl.semaphore_wait(barrier, len(peers))

    sent = []
    ag_copy, tab_copy = {}, {}
    for d in NEAR_FIRST:
        for q, (first, _, _, c0, w) in enumerate(COLORS):
            target = device(**{first: d})
            tab_copy[q, d] = send(
                tables.at[q, (at[first] + d) % RING], seen_tab.at[q, d - 1],
                tab_s.at[q, d - 1], tab_r.at[q, d - 1], target,
            )
            ag_copy[q, d] = send(
                normed.at[:, pl.ds(c0, w)], ag[q].at[d - 1],
                ag_s.at[q, d - 1], ag_r.at[q, d - 1], target,
            )
            sent += [tab_copy[q, d], ag_copy[q, d]]

    row_count = normed.shape[0]
    group = RING * CORES * SLOTS
    numbers = (lax.broadcasted_iota(jnp.int32, (row_count, RING * group), 0) + 1).astype(jnp.float32)

    def table(q, i):
        return tables[q, at[COLORS[q][0]]] if i == 0 else seen_tab[q, i - 1]

    p2_copy = {}
    for i in (0,) + NEAR_FIRST:
        for q, (_, second, _, c0, w) in enumerate(COLORS):
            if i == 0:
                rows = normed[:, c0 : c0 + w]
            else:
                tab_copy[q, i].wait_recv()
                ag_copy[q, i].wait_recv()
                rows = ag[q][i - 1]
            onehot = (numbers == table(q, i)[0:1, :]).astype(jnp.bfloat16)
            picked = lax.dot_general(
                onehot, rows, (((0,), (0,)), ((), ())), preferred_element_type=jnp.float32
            )
            picked = picked.astype(jnp.bfloat16).reshape(RING, RING * CORES, SLOTS, w)
            for b in range(RING):
                pick[q][b, i] = picked[b]
            for d in NEAR_FIRST:
                copy = send(
                    pick[q].at[(at[second] + d) % RING, i], mid[q].at[lead(q, i, d)],
                    p2_s.at[q, d - 1, i], p2_r.at[q, d - 1, i], device(**{second: d}),
                )
                p2_copy[q, d, i] = copy
                sent.append(copy)
            mid[q][lead(q, i, 0)] = pick[q][at[second], i]

    p3_copy = {}
    for q, (_, _, third, c0, w) in enumerate(COLORS):
        for i in (0,) + NEAR_FIRST:
            for d in NEAR_FIRST:
                p2_copy[q, d, i].wait_recv()
        for n, (g, h) in enumerate(PAIRS):
            k = (at[third] + g) % RING * CORES + (core + h) % CORES
            copy = send(
                mid[q].at[:, :, k], piece(arrived, q, g, h),
                p3_s.at[q, n], p3_r.at[q, n], device(h, **{third: g}),
            )
            p3_copy[q, n] = copy
            sent.append(copy)
        piece(arrived, q, 0, 0)[...] = mid[q][:, :, at[third] * CORES + core]

    for load in loads:
        load.wait()
    for q in range(len(COLORS)):
        for n in range(len(PAIRS)):
            p3_copy[q, n].wait_recv()

    width = arrived.shape[-1]
    block = RING * RING * CORES * SLOTS

    @pl.loop(0, RING)
    def _(zi):
        rows = arrived[zi].reshape(block, width)
        gate_part = jnp.dot(rows, v_gate[...], preferred_element_type=jnp.float32)
        up_part = jnp.dot(rows, v_up[...], preferred_element_type=jnp.float32)
        hidden = (gate_part / (1.0 + jnp.exp(-gate_part)) * up_part).astype(jnp.bfloat16)
        done = jnp.dot(hidden, v_down[...], preferred_element_type=jnp.float32)
        result[zi] = done.astype(jnp.bfloat16).reshape(RING, RING, CORES, SLOTS, width)

    r1_copy = {}
    for n, (g, h) in enumerate(PAIRS):
        for q, (_, _, third, c0, w) in enumerate(COLORS):
            copy = send(
                piece(result, q, g, h), back[q].at[:, :, at[third] * CORES + core],
                r1_s.at[q, n], r1_r.at[q, n], device(-h, **{third: -g}),
            )
            r1_copy[q, n] = copy
            sent.append(copy)
    r2_copy = {}
    for q, (_, second, third, c0, w) in enumerate(COLORS):
        back[q][:, :, at[third] * CORES + core] = piece(result, q, 0, 0)[...]
        for n in range(len(PAIRS)):
            r1_copy[q, n].wait_recv()
        for d in NEAR_FIRST:
            src = back[q].at[d] if q == 2 else back[q].at[:, d]
            copy = send(
                src, slots[q].at[:, at[second]],
                r2_s.at[q, d - 1], r2_r.at[q, d - 1], device(**{second: -d}),
            )
            r2_copy[q, d] = copy
            sent.append(copy)
        slots[q][:, at[second]] = back[q][0] if q == 2 else back[q][:, 0]
    r3_copy = {}
    for q, (first, _, _, c0, w) in enumerate(COLORS):
        for d in NEAR_FIRST:
            r2_copy[q, d].wait_recv()
        for i in NEAR_FIRST + (0,):
            rows = slots[q][i].reshape(RING * group, w)
            tab = table(q, i)
            hit = numbers == tab[0:1, :]
            high = jnp.where(hit, tab[1:2, :], 0.0).astype(jnp.bfloat16)
            low = jnp.where(hit, tab[2:3, :], 0.0).astype(jnp.bfloat16)
            some = jnp.dot(high, rows, preferred_element_type=jnp.float32) + jnp.dot(
                low, rows, preferred_element_type=jnp.float32
            )
            if i == 0:
                own_part[:, c0 : c0 + w] = some
            else:
                part[q][i - 1] = some.astype(jnp.bfloat16)
                copy = send(
                    part[q].at[i - 1], got[q].at[i - 1],
                    r3_s.at[q, i - 1], r3_r.at[q, i - 1], device(**{first: -i}),
                )
                r3_copy[q, i] = copy
                sent.append(copy)
    for q, (_, _, _, c0, w) in enumerate(COLORS):
        for i in NEAR_FIRST:
            r3_copy[q, i].wait_recv()
        some = own_part[:, c0 : c0 + w] + base[:, c0 : c0 + w]
        for i in range(RING - 1):
            some = some + got[q][i].astype(jnp.float32)
        out[:, c0 : c0 + w] = some.astype(jnp.bfloat16)
    for copy in sent:
        copy.wait_send()


def routed_layer(normed, tables, base, w_gate, w_up, w_down):
    row_count, width = normed.shape
    hidden = w_gate.shape[1]
    bf16 = jnp.bfloat16
    widths = [c[4] for c in COLORS]

    def per_color(*shape):
        return [pltpu.VMEM(shape + (w,), bf16) for w in widths]

    dma = pltpu.SemaphoreType.DMA
    colors = len(COLORS)
    pairs = len(PAIRS)
    scratch = (
        [
            pltpu.VMEM((width, hidden), bf16),
            pltpu.VMEM((width, hidden), bf16),
            pltpu.VMEM((hidden, width), bf16),
            pltpu.VMEM((colors, RING - 1) + tables.shape[2:], jnp.float32),
            pltpu.VMEM((RING, RING, RING, CORES, SLOTS, width), bf16),
            pltpu.VMEM((RING, RING, RING, CORES, SLOTS, width), bf16),
            pltpu.VMEM((SLOTS, 128), jnp.float32),
            pltpu.VMEM((row_count, width), jnp.float32),
        ]
        + per_color(RING - 1, row_count)
        + per_color(RING, RING, RING * CORES, SLOTS)
        + per_color(RING, RING, RING * CORES, SLOTS)
        + per_color(RING, RING, RING * CORES, SLOTS)
        + per_color(RING, RING, RING * CORES, SLOTS)
        + per_color(RING - 1, row_count)
        + per_color(RING - 1, row_count)
        + [dma((3,))]
        + [dma((colors, RING - 1))] * 4
        + [dma((colors, RING - 1, RING))] * 2
        + [dma((colors, pairs))] * 4
        + [dma((colors, RING - 1))] * 4
    )
    vmem = pl.BlockSpec(memory_space=pltpu.VMEM)
    hbm = pl.BlockSpec(memory_space=pl.ANY)
    return pl.pallas_call(
        moe_kernel,
        out_shape=jax.ShapeDtypeStruct((row_count, width), bf16),
        in_specs=[vmem, vmem, vmem, hbm, hbm, hbm],
        out_specs=vmem,
        scratch_shapes=scratch,
        compiler_params=pltpu.CompilerParams(
            collective_id=0, has_side_effects=True, vmem_limit_bytes=56 * 2**20
        ),
        name="routed_layer",
    )(normed, tables, base, w_gate, w_up, w_down)


def from_behind(block, axis, distance):
    devices = range(lax.axis_size(axis))
    route = [(i - distance, i) for i in devices if i - distance in devices]
    return lax.ppermute(block, axis, route)


def project_norm(conv_out, mix_gain, out_proj):
    values = conv_out.astype(jnp.float32)
    inverse = lax.rsqrt(jnp.mean(values * values, axis=-1) + 1e-06)
    scaled = (values * mix_gain).astype(jnp.bfloat16)
    return jnp.dot(scaled, out_proj, preferred_element_type=jnp.float32) * inverse[:, None]


def swiglu_hidden(row_block, weight_gate, weight_up):
    gate_part = jnp.dot(row_block, weight_gate, preferred_element_type=jnp.float32)
    up_part = jnp.dot(row_block, weight_up, preferred_element_type=jnp.float32)
    return (jax.nn.silu(gate_part) * up_part).astype(jnp.bfloat16)


def body(
    out_gate,
    in_gate,
    conv_values,
    conv_taps,
    mix_gain,
    out_proj,
    residual,
    ffn_gain,
    routes,
    route_weights,
    shared_gate,
    shared_up,
    shared_down,
    expert_gate,
    expert_up,
    expert_down,
):
    mixed_in = in_gate.astype(jnp.float32) * conv_values.astype(jnp.float32)
    taps_count = conv_taps.shape[0]
    length = mixed_in.shape[0]
    earlier = from_behind(mixed_in[length - (taps_count - 1) :], "sp", 1)
    extended = jnp.concatenate([earlier, mixed_in], axis=0)
    filtered = conv_taps[0] * extended[0:length]
    for offset in range(1, taps_count):
        filtered = filtered + conv_taps[offset] * extended[offset : offset + length]
    conv_out = (out_gate.astype(jnp.float32) * filtered).astype(jnp.bfloat16)
    row_count = length // lax.axis_size("tp")
    token_rows = lax.all_to_all(conv_out, "tp", split_axis=0, concat_axis=1, tiled=True)
    mix_result = project_norm(token_rows, mix_gain, out_proj)
    stream = residual.astype(jnp.float32) + mix_result
    norm_inverse = lax.rsqrt(jnp.mean(stream * stream, axis=-1, keepdims=True) + 1e-06)
    normed = (stream * norm_inverse * ffn_gain).astype(jnp.bfloat16)
    shared_result = jnp.dot(
        swiglu_hidden(normed, shared_gate, shared_up),
        shared_down,
        preferred_element_type=jnp.float32,
    )
    experts_total = lax.axis_size("sp") * lax.axis_size("tp")
    tables = slot_tables(routes, route_weights, experts_total)
    base = stream + shared_result
    return routed_layer(normed, tables, base, expert_gate[0], expert_up[0], expert_down[0])


def solution(mesh):
    in_specs = (
        P("sp", "tp"),
        P("sp", "tp"),
        P("sp", "tp"),
        P(None, "tp"),
        P(),
        P(),
        P(("sp", "tp"), None),
        P(),
        P(("sp", "tp"), None),
        P(("sp", "tp"), None),
        P(),
        P(),
        P(),
        P(("sp", "tp"), None, None),
        P(("sp", "tp"), None, None),
        P(("sp", "tp"), None, None),
    )
    out_specs = P(("sp", "tp"), None)
    return jax.shard_map(body, mesh=mesh, in_specs=in_specs, out_specs=out_specs, check_vma=False)
```

```python
import jax
import jax.numpy as jnp
from jax import lax
from jax.experimental import pallas as pl
from jax.experimental.pallas import tpu as pltpu
from jax.sharding import PartitionSpec as P

AXES = ("z", "x", "y")
ORDERS = (("z", "x", "y"), ("x", "y", "z"), ("y", "z", "x"))
CHUNKS = ((384, 384, 384), (256, 256, 384))
RING = 4
CORES = 2
SLOTS = 8
MESH = pl.DeviceIdType.MESH
PAIRS = tuple((g, h) for g in (1, 3, 2, 0) for h in range(CORES) if (g, h) != (0, 0))
NEAR_FIRST = (1, 3, 2)
EPS = 1e-06


def make_lanes():
    lanes, start = [], 0
    for chunk in CHUNKS:
        for color, width in enumerate(chunk):
            lanes.append((color, start, width))
            start += width
    return tuple(lanes)


LANES = make_lanes()
COLORS = len(ORDERS)


def layer_kernel(
    h_out_gate, h_in_gate, h_values, taps, mix_gain, h_proj, h_residual, ffn_gain,
    routes, route_weights, h_sgate, h_sup, h_sdown, h_gate, h_up, h_down,
    out,
    v_out_gate, v_in_gate, v_values, v_proj, v_residual, v_sgate, v_sup, v_sdown,
    v_gate, v_up, v_down,
    mixed, halo, conv, token_rows, base, normed, tables, seen_tab,
    arrived, result, acc_gate, acc_up, hidden, own_part, *rest,
):
    lanes = len(LANES)
    ag, pick, mid, slots, part, got = (rest[n * lanes : (n + 1) * lanes] for n in range(6))
    back = pick
    (load_s, halo_s, halo_r, mix_s, mix_r, tab_s, tab_r, ag_s, ag_r, p2_s, p2_r, p3_s, p3_r,
     r1_s, r1_r, r2_s, r2_r, r3_s, r3_r) = rest[6 * lanes :]
    sp, tp = lax.axis_index("sp"), lax.axis_index("tp")
    sp_count = RING * RING
    at = {"z": sp // RING, "x": sp % RING, "y": tp // CORES}
    core = tp % CORES
    bf16, f32 = jnp.bfloat16, jnp.float32

    def device(core_step=0, **steps):
        p = {k: (at[k] + steps.get(k, 0) + RING) % RING for k in AXES}
        return (p["z"] * RING + p["x"], p["y"] * CORES + (core + core_step + CORES) % CORES)

    def copy_to(src, dst, s, r, target):
        return pltpu.make_async_remote_copy(
            src_ref=src, dst_ref=dst, send_sem=s, recv_sem=r, device_id=target, device_id_type=MESH
        )

    def send(*args):
        copy = copy_to(*args)
        copy.start()
        return copy

    pairs_of_refs = (
        (h_in_gate, v_in_gate), (h_values, v_values), (h_out_gate, v_out_gate),
        (h_proj, v_proj), (h_residual, v_residual), (h_sgate, v_sgate), (h_sup, v_sup),
        (h_sdown, v_sdown), (h_gate, v_gate), (h_up, v_up), (h_down, v_down),
    )
    loads = [
        pltpu.make_async_copy(src, dst, load_s.at[n]) for n, (src, dst) in enumerate(pairs_of_refs)
    ]
    for load in loads:
        load.start()

    barrier = pltpu.get_barrier_semaphore()
    next_sp, last_sp = (sp + 1) % sp_count, (sp + sp_count - 1) % sp_count
    peers = [(next_sp, tp), (last_sp, tp), device(1)] + [
        device(h, **{axis: g}) for axis in AXES for g in range(1, RING) for h in range(CORES)
    ]
    for peer in peers:
        pl.semaphore_signal(barrier, inc=1, device_id=peer, device_id_type=MESH)

    row_count = normed.shape[0]
    channels, length = v_values.shape
    blocks = length // row_count
    for load in loads[0:2]:
        load.wait()
    mixed[:, row_count:] = v_in_gate[...].astype(f32) * v_values[...].astype(f32)
    pl.semaphore_wait(barrier, len(peers))
    halo_copy = send(mixed.at[:, pl.ds(length, row_count)], halo, halo_s, halo_r, (next_sp, tp))
    loads[2].wait()

    tap_columns = []
    for n in range(taps.shape[0]):
        wide = jnp.concatenate(
            [taps[n : n + 1, :], jnp.zeros((1, 2 * row_count - channels), f32)], axis=1
        )
        wide = jnp.broadcast_to(wide, (row_count, 2 * row_count))
        tap_columns.append(jnp.transpose(wide)[0:channels, :])

    def filter_block(j):
        window = mixed[:, j * row_count : (j + 2) * row_count]
        some = tap_columns[0] * pltpu.roll(window, 2, 1)[:, row_count:]
        some = some + tap_columns[1] * pltpu.roll(window, 1, 1)[:, row_count:]
        some = some + tap_columns[2] * window[:, row_count:]
        gate = v_out_gate[:, j * row_count : (j + 1) * row_count].astype(f32)
        conv[j] = (gate * some).astype(bf16)

    for j in range(1, blocks):
        filter_block(j)
    mix_copy = []
    for n, (g, h) in enumerate(PAIRS):
        target = device(h, y=g)
        mix_copy.append(
            copy_to(conv.at[target[1]], token_rows.at[tp], mix_s.at[n], mix_r.at[n], target)
        )

        @pl.when(target[1] != 0)
        def _(copy=mix_copy[n]):
            copy.start()

    experts_total = RING * RING * RING * CORES
    lane = lax.broadcasted_iota(jnp.int32, (row_count, experts_total), 1)
    down_row = lax.broadcasted_iota(jnp.int32, (row_count, experts_total), 0)
    weights = route_weights[...]
    gate_values = weights / jnp.sum(weights, axis=0, keepdims=True) * 2.5
    mask = jnp.zeros((experts_total, row_count), f32)
    gates = jnp.zeros((experts_total, row_count), f32)
    for k in range(routes.shape[0]):
        named = routes[k : k + 1, :] == down_row
        mask = jnp.where(named, 1.0, mask)
        gates = jnp.where(named, gate_values[k : k + 1, :], gates)
    mask, gates = jnp.transpose(mask), jnp.transpose(gates)
    earlier = jnp.where(lane < down_row, 1.0, 0.0).astype(bf16)
    rank = jnp.dot(earlier, mask.astype(bf16), preferred_element_type=f32)
    rank = jnp.where(mask > 0, rank, -1.0)
    numbers_here = (down_row + 1).astype(f32)
    token_list, gate_list = [], []
    for r in range(SLOTS):
        chosen = rank == float(r)
        token_list.append(jnp.sum(jnp.where(chosen, numbers_here, 0.0), axis=0, keepdims=True))
        gate_list.append(jnp.sum(jnp.where(chosen, gates, 0.0), axis=0, keepdims=True))
    token = jnp.concatenate(token_list, axis=0)
    gate = jnp.concatenate(gate_list, axis=0)
    gate_high = gate.astype(bf16)
    gate_low = (gate - gate_high.astype(f32)).astype(bf16)
    listed = (token.astype(bf16), gate_high, gate_low)
    group = RING * CORES * SLOTS
    plane = RING * group
    slot = lax.broadcasted_iota(jnp.int32, (1, RING * plane), 1)
    expert = lax.broadcasted_iota(jnp.int32, (experts_total, RING * plane), 0)
    keep = (
        lax.broadcasted_iota(jnp.int32, (SLOTS, RING * plane), 1) & (SLOTS - 1)
    ) == lax.broadcasted_iota(jnp.int32, (SLOTS, RING * plane), 0)
    for color, (first, second, third) in enumerate(ORDERS):
        digit = {
            first: (slot >> 8) & (RING - 1),
            second: (slot >> 6) & (RING - 1),
            third: (slot >> 4) & (RING - 1),
        }
        expert_of = (digit["z"] << 5) + (digit["x"] << 3) + (digit["y"] << 1)
        expert_of = expert_of + ((slot >> 3) & (CORES - 1))
        spread = jnp.where(expert_of == expert, 1.0, 0.0).astype(bf16)
        for kind, values in enumerate(listed):
            wide = jnp.dot(values, spread, preferred_element_type=f32)
            row = jnp.sum(jnp.where(keep, wide, 0.0), axis=0, keepdims=True)
            for a in range(RING):
                tables[color, a, kind : kind + 1, :] = row[:, a * plane : (a + 1) * plane]
    sent = [halo_copy]
    tab_copy = {}

    def send_tables():
        for d in NEAR_FIRST:
            for color, (first, _, _) in enumerate(ORDERS):
                tab_copy[color, d] = send(
                    tables.at[color, (at[first] + d) % RING], seen_tab.at[color, d - 1],
                    tab_s.at[color, d - 1], tab_r.at[color, d - 1], device(**{first: d}),
                )
                sent.append(tab_copy[color, d])

    halo_copy.wait_recv()
    mixed[:, 0:row_count] = jnp.where(sp == 0, jnp.zeros_like(halo), halo[...])
    filter_block(0)
    for n, (g, h) in enumerate(PAIRS):
        target = device(h, y=g)

        @pl.when(target[1] == 0)
        def _(copy=mix_copy[n]):
            copy.start()

    send_tables()

    loads[3].wait()
    total_channels = blocks * channels

    pair = CORES * channels
    token_rows[tp] = conv[tp]
    squares = jnp.zeros((row_count, 1), f32)
    for g in (0,) + NEAR_FIRST:
        for n in range(len(PAIRS)):
            if PAIRS[n][0] == g:
                mix_copy[n].wait_recv()
        source = (at["y"] - g + RING) % RING
        values = token_rows[pl.ds(source * CORES, CORES)].reshape(pair, row_count)
        values = jnp.transpose(values.astype(f32))
        squares = squares + jnp.sum(values * values, axis=1, keepdims=True)
        step = pair // 128
        gain = jnp.concatenate([mix_gain[pl.ds(source * step + n, 1), :] for n in range(step)], axis=1)
        product = jnp.dot(
            (values * gain).astype(bf16), v_proj[source], preferred_element_type=f32
        )
        if g == 0:
            base[...] = product
        else:
            base[...] += product
    loads[4].wait()
    inverse = lax.rsqrt(squares / total_channels + EPS)
    stream = v_residual[...].astype(f32) + base[...] * inverse
    base[...] = stream
    norm = lax.rsqrt(jnp.mean(stream * stream, axis=1, keepdims=True) + EPS)
    normed[...] = (stream * norm * ffn_gain[...]).astype(bf16)

    def lead(color, i, d):
        return (d, i) if color == 2 else (i, d)

    def piece(ref, lane_at, g, h):
        color, c0, w = LANES[lane_at]
        cols = pl.ds(c0, w)
        if color == 0:
            return ref.at[:, :, g, h, :, cols]
        if color == 1:
            return ref.at[g, :, :, h, :, cols]
        return ref.at[:, g, :, h, :, cols]

    ag_copy = {}
    for d in NEAR_FIRST:
        for q, (color, c0, w) in enumerate(LANES):
            ag_copy[q, d] = send(
                normed.at[:, pl.ds(c0, w)], ag[q].at[d - 1],
                ag_s.at[q, d - 1], ag_r.at[q, d - 1], device(**{ORDERS[color][0]: d}),
            )
            sent.append(ag_copy[q, d])

    numbers = (lax.broadcasted_iota(jnp.int32, (row_count, plane), 0) + 1).astype(f32)

    def table(color, i):
        return tables[color, at[ORDERS[color][0]]] if i == 0 else seen_tab[color, i - 1]

    p2_copy = {}

    def pick_rows(q, i):
        color, c0, w = LANES[q]
        second = ORDERS[color][1]
        if i == 0:
            rows = normed[:, c0 : c0 + w]
        else:
            ag_copy[q, i].wait_recv()
            rows = ag[q][i - 1]
        onehot = jnp.where(numbers == table(color, i)[0:1, :], 1.0, 0.0).astype(bf16)
        picked = lax.dot_general(
            onehot, rows, (((0,), (0,)), ((), ())), preferred_element_type=f32
        )
        picked = picked.astype(bf16).reshape(RING, RING * CORES, SLOTS, w)
        for b in range(RING):
            pick[q][b, i] = picked[b]
        for d in NEAR_FIRST:
            p2_copy[q, d, i] = send(
                pick[q].at[(at[second] + d) % RING, i], mid[q].at[lead(color, i, d)],
                p2_s.at[q, d - 1, i], p2_r.at[q, d - 1, i], device(**{second: d}),
            )
        mid[q][lead(color, i, 0)] = pick[q][at[second], i]

    def swish(gate_part, up_part):
        return (gate_part / (1.0 + jnp.exp(-gate_part)) * up_part).astype(bf16)

    for q in range(lanes):
        pick_rows(q, 0)
    for load in loads[5:8]:
        load.wait()
    rows = normed[...]
    shared = swish(
        jnp.dot(rows, v_sgate[...], preferred_element_type=f32),
        jnp.dot(rows, v_sup[...], preferred_element_type=f32),
    )
    base[...] += jnp.dot(shared, v_sdown[...], preferred_element_type=f32)
    for i in NEAR_FIRST:
        for color in range(COLORS):
            tab_copy[color, i].wait_recv()
        for q in range(lanes):
            pick_rows(q, i)

    p3_copy = {}
    for q, (color, c0, w) in enumerate(LANES):
        third = ORDERS[color][2]
        for i in (0,) + NEAR_FIRST:
            for d in NEAR_FIRST:
                p2_copy[q, d, i].wait()
        for n, (g, h) in enumerate(PAIRS):
            k = (at[third] + g) % RING * CORES + (core + h) % CORES
            p3_copy[q, n] = send(
                mid[q].at[:, :, k], piece(arrived, q, g, h),
                p3_s.at[q, n], p3_r.at[q, n], device(h, **{third: g}),
            )
            sent.append(p3_copy[q, n])
        piece(arrived, q, 0, 0)[...] = mid[q][:, :, at[third] * CORES + core]

    for load in loads[8:]:
        load.wait()
    width = arrived.shape[-1]
    block = RING * RING * CORES * SLOTS
    split = sum(CHUNKS[0])
    half = lanes // 2
    for q in range(half):
        for n in range(len(PAIRS)):
            p3_copy[q, n].wait_recv()

    @pl.loop(0, RING)
    def _(zi):
        rows = arrived[zi, :, :, :, :, 0:split].reshape(block, split)
        acc_gate[zi] = jnp.dot(rows, v_gate[0:split, :], preferred_element_type=f32)
        acc_up[zi] = jnp.dot(rows, v_up[0:split, :], preferred_element_type=f32)

    for q in range(half, lanes):
        for n in range(len(PAIRS)):
            p3_copy[q, n].wait_recv()

    @pl.loop(0, RING)
    def _(zi):
        rows = arrived[zi, :, :, :, :, split:width].reshape(block, width - split)
        gate_part = acc_gate[zi] + jnp.dot(rows, v_gate[split:width, :], preferred_element_type=f32)
        up_part = acc_up[zi] + jnp.dot(rows, v_up[split:width, :], preferred_element_type=f32)
        hidden[zi] = swish(gate_part, up_part)

    r1_copy = {}
    for start, stop, chunk in ((0, split, range(half)), (split, width, range(half, lanes))):

        @pl.loop(0, RING)
        def _(zi):
            done = jnp.dot(hidden[zi], v_down[:, start:stop], preferred_element_type=f32)
            result[zi, :, :, :, :, start:stop] = done.astype(bf16).reshape(
                RING, RING, CORES, SLOTS, stop - start
            )

        for n, (g, h) in enumerate(PAIRS):
            for q in chunk:
                third = ORDERS[LANES[q][0]][2]
                r1_copy[q, n] = send(
                    piece(result, q, g, h), back[q].at[:, :, at[third] * CORES + core],
                    r1_s.at[q, n], r1_r.at[q, n], device(-h, **{third: -g}),
                )
                sent.append(r1_copy[q, n])

    r2_copy = {}
    for q, (color, c0, w) in enumerate(LANES):
        _, second, third = ORDERS[color]
        back[q][:, :, at[third] * CORES + core] = piece(result, q, 0, 0)[...]
        for n in range(len(PAIRS)):
            r1_copy[q, n].wait_recv()
        for d in NEAR_FIRST:
            src = back[q].at[d] if color == 2 else back[q].at[:, d]
            r2_copy[q, d] = send(
                src, slots[q].at[:, at[second]],
                r2_s.at[q, d - 1], r2_r.at[q, d - 1], device(**{second: -d}),
            )
            sent.append(r2_copy[q, d])
        slots[q][:, at[second]] = back[q][0] if color == 2 else back[q][:, 0]
    r3_copy = {}
    for q, (color, c0, w) in enumerate(LANES):
        first = ORDERS[color][0]
        for d in NEAR_FIRST:
            r2_copy[q, d].wait_recv()
        for i in NEAR_FIRST + (0,):
            rows = slots[q][i].reshape(plane, w)
            tab = table(color, i)
            hit = numbers == tab[0:1, :]
            high = jnp.where(hit, tab[1:2, :], 0.0).astype(bf16)
            low = jnp.where(hit, tab[2:3, :], 0.0).astype(bf16)
            some = jnp.dot(high, rows, preferred_element_type=f32) + jnp.dot(
                low, rows, preferred_element_type=f32
            )
            if i == 0:
                own_part[:, c0 : c0 + w] = some
            else:
                part[q][i - 1] = some.astype(bf16)
                r3_copy[q, i] = send(
                    part[q].at[i - 1], got[q].at[i - 1],
                    r3_s.at[q, i - 1], r3_r.at[q, i - 1], device(**{first: -i}),
                )
                sent.append(r3_copy[q, i])
    for q, (_, c0, w) in enumerate(LANES):
        some = own_part[:, c0 : c0 + w] + base[:, c0 : c0 + w]
        for i in NEAR_FIRST:
            r3_copy[q, i].wait_recv()
            some = some + got[q][i - 1].astype(f32)
        out[:, c0 : c0 + w] = some.astype(bf16)
    for copy in sent:
        copy.wait_send()
    for copy in mix_copy:
        copy.wait_send()


def body(
    out_gate, in_gate, conv_values, conv_taps, mix_gain, out_proj, residual, ffn_gain,
    routes, route_weights, shared_gate, shared_up, shared_down,
    expert_gate, expert_up, expert_down,
):
    length, channels = conv_values.shape
    row_count, width = residual.shape
    blocks = length // row_count
    unit = expert_gate.shape[2]
    shared_unit = shared_gate.shape[1]
    bf16, f32 = jnp.bfloat16, jnp.float32
    lanes = len(LANES)
    widths = [w for _, _, w in LANES]

    def per_lane(*shape):
        return [pltpu.VMEM(shape + (w,), bf16) for w in widths]

    def vmem(*shape, dtype=bf16):
        return pltpu.VMEM(shape, dtype)

    dma = pltpu.SemaphoreType.DMA
    near, pairs = RING - 1, len(PAIRS)
    plane = RING * RING * CORES * SLOTS
    scratch = (
        [vmem(channels, length)] * 3
        + [vmem(RING, CORES * channels, width), vmem(row_count, width)]
        + [vmem(width, shared_unit), vmem(width, shared_unit), vmem(shared_unit, width)]
        + [vmem(width, unit), vmem(width, unit), vmem(unit, width)]
        + [vmem(channels, row_count + length, dtype=f32), vmem(channels, row_count, dtype=f32)]
        + [vmem(blocks, channels, row_count)] * 2
        + [vmem(row_count, width, dtype=f32), vmem(row_count, width)]
        + [vmem(COLORS, RING, 8, plane, dtype=f32), vmem(COLORS, near, 8, plane, dtype=f32)]
        + [vmem(RING, RING, RING, CORES, SLOTS, width)] * 2
        + [vmem(RING, plane, unit, dtype=f32)] * 2
        + [vmem(RING, plane, unit), vmem(row_count, width, dtype=f32)]
        + per_lane(near, row_count)
        + per_lane(RING, RING, RING * CORES, SLOTS)
        + per_lane(RING, RING, RING * CORES, SLOTS)
        + per_lane(RING, RING, RING * CORES, SLOTS)
        + per_lane(near, row_count)
        + per_lane(near, row_count)
        + [dma((11,)), dma, dma, dma((pairs,)), dma((pairs,))]
        + [dma((COLORS, near))] * 2
        + [dma((lanes, near))] * 2
        + [dma((lanes, near, RING))] * 2
        + [dma((lanes, pairs))] * 4
        + [dma((lanes, near))] * 4
    )
    whole = pl.BlockSpec(memory_space=pltpu.VMEM)
    hbm = pl.BlockSpec(memory_space=pl.ANY)
    return pl.pallas_call(
        layer_kernel,
        out_shape=jax.ShapeDtypeStruct((row_count, width), bf16),
        in_specs=[hbm, hbm, hbm, whole, whole, hbm, hbm, whole, whole, whole] + [hbm] * 6,
        out_specs=whole,
        scratch_shapes=scratch,
        compiler_params=pltpu.CompilerParams(
            collective_id=0, has_side_effects=True, vmem_limit_bytes=67043328
        ),
        name="whole_layer",
    )(
        out_gate.T, in_gate.T, conv_values.T, conv_taps, mix_gain.reshape(-1, 128),
        out_proj.reshape(RING, CORES * channels, width), residual, ffn_gain.reshape(1, width),
        routes.T, route_weights.T, shared_gate, shared_up, shared_down,
        expert_gate[0], expert_up[0], expert_down[0],
    )


def solution(mesh):
    in_specs = (
        P("sp", "tp"),
        P("sp", "tp"),
        P("sp", "tp"),
        P(None, "tp"),
        P(),
        P(),
        P(("sp", "tp"), None),
        P(),
        P(("sp", "tp"), None),
        P(("sp", "tp"), None),
        P(),
        P(),
        P(),
        P(("sp", "tp"), None, None),
        P(("sp", "tp"), None, None),
        P(("sp", "tp"), None, None),
    )
    out_specs = P(("sp", "tp"), None)
    return jax.shard_map(body, mesh=mesh, in_specs=in_specs, out_specs=out_specs, check_vma=False)
```

```python
import jax
import jax.numpy as jnp
from jax import lax
from jax.experimental import pallas as pl
from jax.experimental.pallas import tpu as pltpu
from jax.sharding import PartitionSpec as P

AXES = ("z", "x", "y")
ORDERS = (("z", "x", "y"), ("x", "y", "z"), ("y", "z", "x"))
CHUNKS = ((256, 256, 256), (256, 256, 256), (128, 128, 256))
RING = 4
CORES = 2
SLOTS = 8
MESH = pl.DeviceIdType.MESH
PAIRS = tuple((g, h) for g in (2, 1, 3, 0) for h in range(CORES) if (g, h) != (0, 0))
NEAR_FIRST = (1, 3, 2)
FAR_FIRST = (2, 1, 3)
EPS = 1e-06


def make_lanes():
    lanes, start = [], 0
    for chunk in CHUNKS:
        for color, width in enumerate(chunk):
            lanes.append((color, start, width))
            start += width
    return tuple(lanes)


LANES = make_lanes()
CHUNK_ENDS = tuple(sum(sum(c) for c in CHUNKS[: n + 1]) for n in range(len(CHUNKS)))
COLORS = len(ORDERS)


def layer_kernel(
    h_out_gate, h_in_gate, h_values, h_taps, h_mix_gain, h_proj, h_residual, h_ffn_gain,
    h_routes, h_route_weights, h_sgate, h_sup, h_sdown, h_gate, h_up, h_down,
    out,
    v_out, taps, mix_gain, ffn_gain, routes, route_weights,
    v_out_gate, v_in_gate, v_values, v_proj, v_residual, v_sgate, v_sup, v_sdown,
    v_gate, v_up, v_down,
    mixed, halo_out, halo, conv, token_rows, base, normed, tables, seen_tab,
    arrived, result, acc_gate, acc_up, hidden, own_part, *rest,
):
    lanes = len(LANES)
    ag, pick, mid, slots, part, got = (rest[n * lanes : (n + 1) * lanes] for n in range(6))
    back = pick
    (load_s, halo_s, halo_r, mix_s, mix_r, tab_s, tab_r, ag_s, ag_r, p2_s, p2_r, p3_s, p3_r,
     r1_s, r1_r, r2_s, r2_r, r3_s, r3_r, out_s) = rest[6 * lanes :]
    sp, tp = lax.axis_index("sp"), lax.axis_index("tp")
    sp_count = RING * RING
    at = {"z": sp // RING, "x": sp % RING, "y": tp // CORES}
    core = tp % CORES
    bf16, f32 = jnp.bfloat16, jnp.float32

    def device(core_step=0, **steps):
        p = {k: (at[k] + steps.get(k, 0) + RING) % RING for k in AXES}
        return (p["z"] * RING + p["x"], p["y"] * CORES + (core + core_step + CORES) % CORES)

    def copy_to(src, dst, s, r, target):
        return pltpu.make_async_remote_copy(
            src_ref=src, dst_ref=dst, send_sem=s, recv_sem=r, device_id=target, device_id_type=MESH
        )

    def send(*args):
        copy = copy_to(*args)
        copy.start()
        return copy

    pairs_of_refs = (
        (h_routes, routes), (h_route_weights, route_weights), (h_in_gate, v_in_gate),
        (h_values, v_values), (h_taps, taps), (h_out_gate, v_out_gate),
        (h_mix_gain, mix_gain), (h_proj, v_proj), (h_residual, v_residual),
        (h_ffn_gain, ffn_gain), (h_sgate, v_sgate), (h_sup, v_sup), (h_sdown, v_sdown),
        (h_gate, v_gate), (h_up, v_up), (h_down, v_down),
    )
    loads = [
        pltpu.make_async_copy(src, dst, load_s.at[n]) for n, (src, dst) in enumerate(pairs_of_refs)
    ]

    def drain(ref, semaphore):
        pltpu.make_async_copy(ref, ref, semaphore).wait()

    barrier = pltpu.get_barrier_semaphore()
    next_sp, last_sp = (sp + 1) % sp_count, (sp + sp_count - 1) % sp_count
    peers = [(next_sp, tp), (last_sp, tp), device(1)] + [
        device(h, **{axis: g}) for axis in AXES for g in range(1, RING) for h in range(CORES)
    ]
    for peer in peers:
        pl.semaphore_signal(barrier, inc=1, device_id=peer, device_id_type=MESH)

    for load in loads[0:6]:
        load.start()
    row_count = normed.shape[0]
    channels, length = v_values.shape
    blocks = length // row_count
    for load in loads[2:6]:
        load.wait()
    for load in loads[6:]:
        load.start()
    mixed[:, row_count:] = v_in_gate[...].astype(f32) * v_values[...].astype(f32)
    spare = 2 * row_count - channels
    tail = jnp.concatenate(
        [mixed[:, length : length + row_count], jnp.zeros((spare, row_count), f32)], axis=0
    )
    halo_out[...] = jnp.transpose(tail)[row_count - 8 :, :]
    tap_columns = []
    for n in range(taps.shape[0]):
        wide = jnp.concatenate(
            [taps[n : n + 1, :], jnp.zeros((1, 2 * row_count - channels), f32)], axis=1
        )
        wide = jnp.broadcast_to(wide, (row_count, 2 * row_count))
        tap_columns.append(jnp.transpose(wide)[0:channels, :])

    def filter_block(j):
        window = mixed[:, j * row_count : (j + 2) * row_count]
        some = tap_columns[0] * pltpu.roll(window, 2, 1)[:, row_count:]
        some = some + tap_columns[1] * pltpu.roll(window, 1, 1)[:, row_count:]
        some = some + tap_columns[2] * window[:, row_count:]
        gate = v_out_gate[:, j * row_count : (j + 1) * row_count].astype(f32)
        conv[j] = (gate * some).astype(bf16)

    for j in range(1, blocks):
        filter_block(j)
    pl.semaphore_wait(barrier, len(peers))
    halo_copy = send(halo_out, halo, halo_s, halo_r, (next_sp, tp))

    def mix_sends(zero):
        for g, h in PAIRS:
            target = device(h, y=g)
            copy = copy_to(conv.at[target[1]], token_rows.at[tp], mix_s, mix_r.at[g], target)

            @pl.when((target[1] == 0) == zero)
            def _(copy=copy):
                copy.start()

    mix_sends(False)
    halo_copy.wait()
    late = jnp.concatenate(
        [jnp.zeros((row_count - 8, 2 * row_count), f32), halo[...]], axis=0
    )
    late = jnp.transpose(late)[0:channels, :]
    mixed[:, 0:row_count] = jnp.where(sp == 0, jnp.zeros_like(late), late)
    filter_block(0)
    mix_sends(True)

    for load in loads[0:2]:
        load.wait()
    experts_total = RING * RING * RING * CORES
    lane = lax.broadcasted_iota(jnp.int32, (row_count, experts_total), 1)
    down_row = lax.broadcasted_iota(jnp.int32, (row_count, experts_total), 0)
    weights = route_weights[...]
    gate_values = weights / jnp.sum(weights, axis=0, keepdims=True) * 2.5
    mask = jnp.zeros((experts_total, row_count), f32)
    gates = jnp.zeros((experts_total, row_count), f32)
    for k in range(routes.shape[0]):
        named = routes[k : k + 1, :] == down_row
        mask = jnp.where(named, 1.0, mask)
        gates = jnp.where(named, gate_values[k : k + 1, :], gates)
    mask, gates = jnp.transpose(mask), jnp.transpose(gates)
    earlier = jnp.where(lane < down_row, 1.0, 0.0).astype(bf16)
    rank = jnp.dot(earlier, mask.astype(bf16), preferred_element_type=f32)
    rank = jnp.where(mask > 0, rank, -1.0)
    numbers_here = (down_row + 1).astype(f32)
    token_list, gate_list = [], []
    for r in range(SLOTS):
        chosen = rank == float(r)
        token_list.append(jnp.sum(jnp.where(chosen, numbers_here, 0.0), axis=0, keepdims=True))
        gate_list.append(jnp.sum(jnp.where(chosen, gates, 0.0), axis=0, keepdims=True))
    token = jnp.concatenate(token_list, axis=0)
    gate = jnp.concatenate(gate_list, axis=0)
    gate_high = gate.astype(bf16)
    gate_low = (gate - gate_high.astype(f32)).astype(bf16)
    listed = (token.astype(bf16), gate_high, gate_low)
    group = RING * CORES * SLOTS
    plane = RING * group
    slot = lax.broadcasted_iota(jnp.int32, (1, RING * plane), 1)
    expert = lax.broadcasted_iota(jnp.int32, (experts_total, RING * plane), 0)
    keep = (
        lax.broadcasted_iota(jnp.int32, (SLOTS, RING * plane), 1) & (SLOTS - 1)
    ) == lax.broadcasted_iota(jnp.int32, (SLOTS, RING * plane), 0)
    for color, (first, second, third) in enumerate(ORDERS):
        digit = {
            first: (slot >> 8) & (RING - 1),
            second: (slot >> 6) & (RING - 1),
            third: (slot >> 4) & (RING - 1),
        }
        expert_of = (digit["z"] << 5) + (digit["x"] << 3) + (digit["y"] << 1)
        expert_of = expert_of + ((slot >> 3) & (CORES - 1))
        spread = jnp.where(expert_of == expert, 1.0, 0.0).astype(bf16)
        for kind, values in enumerate(listed):
            wide = jnp.dot(values, spread, preferred_element_type=f32)
            row = jnp.sum(jnp.where(keep, wide, 0.0), axis=0, keepdims=True)
            for a in range(RING):
                tables[color, a, kind : kind + 1, :] = row[:, a * plane : (a + 1) * plane]
    for d in FAR_FIRST:
        for color, (first, _, _) in enumerate(ORDERS):
            send(
                tables.at[color, (at[first] + d) % RING], seen_tab.at[d - 1, color],
                tab_s, tab_r.at[d - 1], device(**{first: d}),
            )

    for load in loads[6:8]:
        load.wait()
    total_channels = blocks * channels

    pair = CORES * channels
    token_rows[tp] = conv[tp]
    squares = jnp.zeros((row_count, 1), f32)
    for g in (0,) + NEAR_FIRST:
        drain(token_rows.at[pl.ds(0, CORES if g else 1)], mix_r.at[g])
        source = (at["y"] - g + RING) % RING
        values = token_rows[pl.ds(source * CORES, CORES)].reshape(pair, row_count)
        values = jnp.transpose(values.astype(f32))
        squares = squares + jnp.sum(values * values, axis=1, keepdims=True)
        step = pair // 128
        gain = jnp.concatenate([mix_gain[pl.ds(source * step + n, 1), :] for n in range(step)], axis=1)
        product = jnp.dot(
            (values * gain).astype(bf16), v_proj[source], preferred_element_type=f32
        )
        if g == 0:
            base[...] = product
        else:
            base[...] += product
    for load in loads[8:10]:
        load.wait()
    inverse = lax.rsqrt(squares / total_channels + EPS)
    stream = v_residual[...].astype(f32) + base[...] * inverse
    base[...] = stream
    norm = lax.rsqrt(jnp.mean(stream * stream, axis=1, keepdims=True) + EPS)
    normed[...] = (stream * norm * ffn_gain[...]).astype(bf16)

    def lead(color, i, d):
        return (d, i) if color == 2 else (i, d)

    def piece(ref, lane_at, g, h):
        color, c0, w = LANES[lane_at]
        cols = pl.ds(c0, w)
        if color == 0:
            return ref.at[:, :, g, h, :, cols]
        if color == 1:
            return ref.at[g, :, :, h, :, cols]
        return ref.at[:, g, :, h, :, cols]

    def gather_send(q, d, src, s):
        color = LANES[q][0]
        step = 1 if d == 1 or (d == 2 and q % 2 == 0) else -1
        send(src, ag[q].at[d - 1], s, ag_r.at[q, d - 1], device(**{ORDERS[color][0]: step}))

    for d in (1, 3):
        for q, (_, c0, w) in enumerate(LANES):
            gather_send(q, d, normed.at[:, pl.ds(c0, w)], ag_s.at[d - 1])

    numbers = (lax.broadcasted_iota(jnp.int32, (row_count, plane), 0) + 1).astype(f32)

    def table(color, i):
        return tables[color, at[ORDERS[color][0]]] if i == 0 else seen_tab[i - 1, color]

    def pick_rows(q, i):
        color, c0, w = LANES[q]
        second = ORDERS[color][1]
        if i == 0:
            rows = normed[:, c0 : c0 + w]
        else:
            drain(ag[q].at[i - 1], ag_r.at[q, i - 1])
            if i == (3 if q % 2 else 1):
                gather_send(q, 2, ag[q].at[i - 1], ag_s.at[1])
            rows = ag[q][i - 1]
        onehot = jnp.where(numbers == table(color, i)[0:1, :], 1.0, 0.0).astype(bf16)
        picked = lax.dot_general(
            onehot, rows, (((0,), (0,)), ((), ())), preferred_element_type=f32
        )
        picked = picked.astype(bf16).reshape(RING, RING * CORES, SLOTS, w)
        for b in range(RING):
            pick[q][b, i] = picked[b]
        for d in FAR_FIRST:
            send(
                pick[q].at[(at[second] + d) % RING, i], mid[q].at[lead(color, i, d)],
                p2_s.at[q], p2_r.at[q], device(**{second: d}),
            )
        mid[q][lead(color, i, 0)] = pick[q][at[second], i]

    def swish(gate_part, up_part):
        return (gate_part / (1.0 + jnp.exp(-gate_part)) * up_part).astype(bf16)

    for q in range(lanes):
        pick_rows(q, 0)
    for load in loads[10:13]:
        load.wait()
    rows = normed[...]
    shared = swish(
        jnp.dot(rows, v_sgate[...], preferred_element_type=f32),
        jnp.dot(rows, v_sup[...], preferred_element_type=f32),
    )
    base[...] += jnp.dot(shared, v_sdown[...], preferred_element_type=f32)
    for i in NEAR_FIRST:
        drain(seen_tab.at[i - 1], tab_r.at[i - 1])
    for turn in ((1, 3), (3, 1), (2, 2)):
        for q in range(lanes):
            pick_rows(q, turn[q % 2])

    near, pairs = RING - 1, len(PAIRS)
    for q, (color, c0, w) in enumerate(LANES):
        third = ORDERS[color][2]
        drain(mid[q].at[pl.ds(0, near)], p2_r.at[q])
        drain(pick[q].at[pl.ds(0, near)], p2_s.at[q])
        for g, h in PAIRS:
            k = (at[third] + g) % RING * CORES + (core + h) % CORES
            send(
                mid[q].at[:, :, k], piece(arrived, q, g, h),
                p3_s.at[q], p3_r.at[q], device(h, **{third: g}),
            )
        piece(arrived, q, 0, 0)[...] = mid[q][:, :, at[third] * CORES + core]

    for load in loads[13:]:
        load.wait()
    width = arrived.shape[-1]
    block = RING * RING * CORES * SLOTS
    spans = tuple(zip((0,) + CHUNK_ENDS, CHUNK_ENDS))
    for chunk, (start, stop) in enumerate(spans):
        for q in range(chunk * COLORS, (chunk + 1) * COLORS):
            drain(mid[q].at[:, :, pl.ds(0, pairs)], p3_r.at[q])

        @pl.loop(0, RING)
        def _(zi):
            rows = arrived[zi, :, :, :, :, start:stop].reshape(block, stop - start)
            gate_part = jnp.dot(rows, v_gate[start:stop, :], preferred_element_type=f32)
            up_part = jnp.dot(rows, v_up[start:stop, :], preferred_element_type=f32)
            if chunk > 0:
                gate_part = gate_part + acc_gate[zi]
                up_part = up_part + acc_up[zi]
            if chunk + 1 == len(spans):
                hidden[zi] = swish(gate_part, up_part)
            else:
                acc_gate[zi] = gate_part
                acc_up[zi] = up_part

    for chunk, (start, stop) in enumerate(spans):

        @pl.loop(0, RING)
        def _(zi):
            done = jnp.dot(hidden[zi], v_down[:, start:stop], preferred_element_type=f32)
            result[zi, :, :, :, :, start:stop] = done.astype(bf16).reshape(
                RING, RING, CORES, SLOTS, stop - start
            )

        for color in range(COLORS):
            q = chunk * COLORS + color
            third = ORDERS[color][2]
            for g, h in PAIRS:
                send(
                    piece(result, q, g, h), back[q].at[:, :, at[third] * CORES + core],
                    r1_s.at[q], r1_r.at[q], device(-h, **{third: -g}),
                )

    for q, (color, c0, w) in enumerate(LANES):
        _, second, third = ORDERS[color]
        back[q][:, :, at[third] * CORES + core] = piece(result, q, 0, 0)[...]
        drain(back[q].at[:, :, pl.ds(0, pairs)], r1_r.at[q])
        for d in FAR_FIRST:
            src = back[q].at[d] if color == 2 else back[q].at[:, d]
            send(
                src, slots[q].at[:, at[second]], r2_s.at[q], r2_r.at[q], device(**{second: -d})
            )
        slots[q][:, at[second]] = back[q][0] if color == 2 else back[q][:, 0]
    for q, (color, c0, w) in enumerate(LANES):
        first = ORDERS[color][0]
        drain(slots[q].at[:, pl.ds(0, near)], r2_r.at[q])
        for i in FAR_FIRST + (0,):
            rows = slots[q][i].reshape(plane, w)
            tab = table(color, i)
            hit = numbers == tab[0:1, :]
            high = jnp.where(hit, tab[1:2, :], 0.0).astype(bf16)
            low = jnp.where(hit, tab[2:3, :], 0.0).astype(bf16)
            some = jnp.dot(high, rows, preferred_element_type=f32) + jnp.dot(
                low, rows, preferred_element_type=f32
            )
            if i == 0:
                own_part[:, c0 : c0 + w] = some
            else:
                part[q][i - 1] = some.astype(bf16)
                send(
                    part[q].at[i - 1], got[q].at[i - 1], r3_s.at[q], r3_r.at[q],
                    device(**{first: -i}),
                )
    for q, (_, c0, w) in enumerate(LANES):
        some = own_part[:, c0 : c0 + w] + base[:, c0 : c0 + w]
        drain(got[q], r3_r.at[q])
        for i in range(near):
            some = some + got[q][i].astype(f32)
        v_out[:, c0 : c0 + w] = some.astype(bf16)
        cols = pl.ds(c0, w)
        pltpu.make_async_copy(v_out.at[:, cols], out.at[:, cols], out_s).start()
    drain(conv.at[pl.ds(0, pairs)], mix_s)
    drain(seen_tab, tab_s)
    for n in range(near):
        drain(normed, ag_s.at[n])
    for q in range(lanes):
        drain(mid[q].at[:, :, pl.ds(0, pairs)], p3_s.at[q])
        drain(back[q].at[:, :, pl.ds(0, pairs)], r1_s.at[q])
        drain(slots[q].at[:, pl.ds(0, near)], r2_s.at[q])
        drain(part[q], r3_s.at[q])
    drain(v_out, out_s)


def body(
    out_gate, in_gate, conv_values, conv_taps, mix_gain, out_proj, residual, ffn_gain,
    routes, route_weights, shared_gate, shared_up, shared_down,
    expert_gate, expert_up, expert_down,
):
    length, channels = conv_values.shape
    row_count, width = residual.shape
    blocks = length // row_count
    unit = expert_gate.shape[2]
    shared_unit = shared_gate.shape[1]
    bf16, f32 = jnp.bfloat16, jnp.float32
    lanes = len(LANES)
    widths = [w for _, _, w in LANES]

    def per_lane(*shape):
        return [pltpu.VMEM(shape + (w,), bf16) for w in widths]

    def vmem(*shape, dtype=bf16):
        return pltpu.VMEM(shape, dtype)

    dma = pltpu.SemaphoreType.DMA
    near, pairs = RING - 1, len(PAIRS)
    plane = RING * RING * CORES * SLOTS
    mix_gain, ffn_gain = mix_gain.reshape(-1, 128), ffn_gain.reshape(1, width)
    routes, route_weights = routes.T, route_weights.T
    small = (conv_taps, mix_gain, ffn_gain, routes, route_weights)
    scratch = (
        [vmem(row_count, width)]
        + [vmem(*a.shape, dtype=a.dtype) for a in small]
        + [vmem(channels, length)] * 3
        + [vmem(RING, CORES * channels, width), vmem(row_count, width)]
        + [vmem(width, shared_unit), vmem(width, shared_unit), vmem(shared_unit, width)]
        + [vmem(width, unit), vmem(width, unit), vmem(unit, width)]
        + [vmem(channels, row_count + length, dtype=f32), vmem(8, 2 * row_count, dtype=f32)]
        + [vmem(8, 2 * row_count, dtype=f32)]
        + [vmem(blocks, channels, row_count)] * 2
        + [vmem(row_count, width, dtype=f32), vmem(row_count, width)]
        + [vmem(COLORS, RING, 8, plane, dtype=f32), vmem(near, COLORS, 8, plane, dtype=f32)]
        + [vmem(RING, RING, RING, CORES, SLOTS, width)] * 2
        + [vmem(RING, plane, unit, dtype=f32)] * 2
        + [vmem(RING, plane, unit), vmem(row_count, width, dtype=f32)]
        + per_lane(near, row_count)
        + per_lane(RING, RING, RING * CORES, SLOTS)
        + per_lane(RING, RING, RING * CORES, SLOTS)
        + per_lane(RING, RING, RING * CORES, SLOTS)
        + per_lane(near, row_count)
        + per_lane(near, row_count)
        + [dma((16,)), dma, dma, dma, dma((RING,)), dma, dma((near,)), dma((near,))]
        + [dma((lanes, near))]
        + [dma((lanes,))] * 10
        + [dma]
    )
    hbm = pl.BlockSpec(memory_space=pl.ANY)
    return pl.pallas_call(
        layer_kernel,
        out_shape=jax.ShapeDtypeStruct((row_count, width), bf16),
        in_specs=[hbm] * 16,
        out_specs=hbm,
        scratch_shapes=scratch,
        compiler_params=pltpu.CompilerParams(
            collective_id=0, has_side_effects=True, vmem_limit_bytes=67043328
        ),
        name="whole_layer",
    )(
        out_gate.T, in_gate.T, conv_values.T, conv_taps, mix_gain,
        out_proj.reshape(RING, CORES * channels, width), residual, ffn_gain,
        routes, route_weights, shared_gate, shared_up, shared_down,
        expert_gate[0], expert_up[0], expert_down[0],
    )


def solution(mesh):
    in_specs = (
        P("sp", "tp"),
        P("sp", "tp"),
        P("sp", "tp"),
        P(None, "tp"),
        P(),
        P(),
        P(("sp", "tp"), None),
        P(),
        P(("sp", "tp"), None),
        P(("sp", "tp"), None),
        P(),
        P(),
        P(),
        P(("sp", "tp"), None, None),
        P(("sp", "tp"), None, None),
        P(("sp", "tp"), None, None),
    )
    out_specs = P(("sp", "tp"), None)
    return jax.shard_map(body, mesh=mesh, in_specs=in_specs, out_specs=out_specs, check_vma=False)
```

```python
import jax
import jax.numpy as jnp
from jax import lax
from jax.experimental import pallas as pl
from jax.experimental.pallas import tpu as pltpu
from jax.sharding import PartitionSpec as P

AXES = ("z", "x", "y")
ORDERS = (("z", "x", "y"), ("x", "y", "z"), ("y", "z", "x"))
CHUNKS = ((128, 128, 256), (256, 256, 128), (128, 128, 256), (128, 128, 128))
RING = 4
CORES = 2
SLOTS = 8
MESH = pl.DeviceIdType.MESH
PAIRS = tuple((g, h) for g in (2, 1, 3, 0) for h in range(CORES) if (g, h) != (0, 0))
NEAR_FIRST = (1, 3, 2)
FAR_FIRST = (2, 1, 3)
EPS = 1e-06


def make_lanes():
    lanes, start = [], 0
    for chunk in CHUNKS:
        for color, width in enumerate(chunk):
            lanes.append((color, start, width))
            start += width
    return tuple(lanes)


LANES = make_lanes()
CHUNK_ENDS = tuple(sum(sum(c) for c in CHUNKS[: n + 1]) for n in range(len(CHUNKS)))
COLORS = len(ORDERS)


def layer_kernel(
    h_out_gate, h_in_gate, h_values, h_taps, h_mix_gain, h_proj, h_residual, h_ffn_gain,
    h_routes, h_route_weights, h_sgate, h_sup, h_sdown, h_gate, h_up, h_down,
    out,
    v_out, taps, mix_gain, ffn_gain, routes, route_weights,
    v_out_gate, v_in_gate, v_values, v_proj, v_residual, v_sgate, v_sup, v_sdown,
    v_gate, v_up, v_down,
    mixed, halo_out, halo, conv, token_rows, base, normed, tables, seen_tab,
    arrived, result, acc_gate, acc_up, hidden, own_part, *rest,
):
    lanes = len(LANES)
    ag, pick, mid, slots, part, got = (rest[n * lanes : (n + 1) * lanes] for n in range(6))
    back = pick
    (load_s, halo_s, halo_r, mix_s, mix_r, tab_s, tab_r, ag_s, ag_r, p2_s, p2_r, p3_s, p3_r,
     r1_s, r1_r, r2_s, r2_r, r3_s, r3_r, out_s) = rest[6 * lanes :]
    sp, tp = lax.axis_index("sp"), lax.axis_index("tp")
    sp_count = RING * RING
    at = {"z": sp // RING, "x": sp % RING, "y": tp // CORES}
    core = tp % CORES
    bf16, f32 = jnp.bfloat16, jnp.float32

    def device(core_step=0, **steps):
        p = {k: (at[k] + steps.get(k, 0) + RING) % RING for k in AXES}
        return (p["z"] * RING + p["x"], p["y"] * CORES + (core + core_step + CORES) % CORES)

    def copy_to(src, dst, s, r, target):
        return pltpu.make_async_remote_copy(
            src_ref=src, dst_ref=dst, send_sem=s, recv_sem=r, device_id=target, device_id_type=MESH
        )

    def send(*args):
        copy = copy_to(*args)
        copy.start()
        return copy

    pairs_of_refs = (
        (h_routes, routes), (h_route_weights, route_weights), (h_in_gate, v_in_gate),
        (h_values, v_values), (h_taps, taps), (h_out_gate, v_out_gate),
        (h_mix_gain, mix_gain), (h_proj, v_proj), (h_residual, v_residual),
        (h_ffn_gain, ffn_gain), (h_sgate, v_sgate), (h_sup, v_sup), (h_sdown, v_sdown),
        (h_gate, v_gate), (h_up, v_up), (h_down, v_down),
    )
    loads = [
        pltpu.make_async_copy(src, dst, load_s.at[n]) for n, (src, dst) in enumerate(pairs_of_refs)
    ]

    def drain(ref, semaphore):
        pltpu.make_async_copy(ref, ref, semaphore).wait()

    barrier = pltpu.get_barrier_semaphore()
    next_sp, last_sp = (sp + 1) % sp_count, (sp + sp_count - 1) % sp_count
    peers = [(next_sp, tp), (last_sp, tp), device(1)] + [
        device(h, **{axis: g}) for axis in AXES for g in range(1, RING) for h in range(CORES)
    ]
    for peer in peers:
        pl.semaphore_signal(barrier, inc=1, device_id=peer, device_id_type=MESH)

    for load in loads[0:6]:
        load.start()
    row_count = normed.shape[0]
    channels, length = v_values.shape
    blocks = length // row_count
    for load in loads[2:6]:
        load.wait()
    for load in loads[6:]:
        load.start()
    mixed[:, row_count:] = v_in_gate[...].astype(f32) * v_values[...].astype(f32)
    spare = 2 * row_count - channels
    tail = jnp.concatenate(
        [mixed[:, length : length + row_count], jnp.zeros((spare, row_count), f32)], axis=0
    )
    halo_out[...] = jnp.transpose(tail)[row_count - 8 :, :]
    tap_columns = []
    for n in range(taps.shape[0]):
        wide = jnp.concatenate(
            [taps[n : n + 1, :], jnp.zeros((1, 2 * row_count - channels), f32)], axis=1
        )
        wide = jnp.broadcast_to(wide, (row_count, 2 * row_count))
        tap_columns.append(jnp.transpose(wide)[0:channels, :])

    def filter_block(j):
        window = mixed[:, j * row_count : (j + 2) * row_count]
        some = tap_columns[0] * pltpu.roll(window, 2, 1)[:, row_count:]
        some = some + tap_columns[1] * pltpu.roll(window, 1, 1)[:, row_count:]
        some = some + tap_columns[2] * window[:, row_count:]
        gate = v_out_gate[:, j * row_count : (j + 1) * row_count].astype(f32)
        conv[j] = (gate * some).astype(bf16)

    for j in range(1, blocks):
        filter_block(j)
    pl.semaphore_wait(barrier, len(peers))
    halo_copy = send(halo_out, halo, halo_s, halo_r, (next_sp, tp))

    def mix_sends(zero):
        for g, h in PAIRS:
            target = device(h, y=g)
            copy = copy_to(conv.at[target[1]], token_rows.at[tp], mix_s, mix_r.at[g], target)

            @pl.when((target[1] == 0) == zero)
            def _(copy=copy):
                copy.start()

    mix_sends(False)
    halo_copy.wait()
    late = jnp.concatenate(
        [jnp.zeros((row_count - 8, 2 * row_count), f32), halo[...]], axis=0
    )
    late = jnp.transpose(late)[0:channels, :]
    mixed[:, 0:row_count] = jnp.where(sp == 0, jnp.zeros_like(late), late)
    filter_block(0)
    mix_sends(True)

    for load in loads[0:2]:
        load.wait()
    experts_total = RING * RING * RING * CORES
    lane = lax.broadcasted_iota(jnp.int32, (row_count, experts_total), 1)
    down_row = lax.broadcasted_iota(jnp.int32, (row_count, experts_total), 0)
    weights = route_weights[...]
    gate_values = weights / jnp.sum(weights, axis=0, keepdims=True) * 2.5
    mask = jnp.zeros((experts_total, row_count), f32)
    gates = jnp.zeros((experts_total, row_count), f32)
    for k in range(routes.shape[0]):
        named = routes[k : k + 1, :] == down_row
        mask = jnp.where(named, 1.0, mask)
        gates = jnp.where(named, gate_values[k : k + 1, :], gates)
    mask, gates = jnp.transpose(mask), jnp.transpose(gates)
    earlier = jnp.where(lane < down_row, 1.0, 0.0).astype(bf16)
    rank = jnp.dot(earlier, mask.astype(bf16), preferred_element_type=f32)
    rank = jnp.where(mask > 0, rank, -1.0)
    numbers_here = (down_row + 1).astype(f32)
    token_list, gate_list = [], []
    for r in range(SLOTS):
        chosen = rank == float(r)
        token_list.append(jnp.sum(jnp.where(chosen, numbers_here, 0.0), axis=0, keepdims=True))
        gate_list.append(jnp.sum(jnp.where(chosen, gates, 0.0), axis=0, keepdims=True))
    token = jnp.concatenate(token_list, axis=0)
    gate = jnp.concatenate(gate_list, axis=0)
    gate_high = gate.astype(bf16)
    gate_low = (gate - gate_high.astype(f32)).astype(bf16)
    listed = (token.astype(bf16), gate_high, gate_low)
    group = RING * CORES * SLOTS
    plane = RING * group
    slot = lax.broadcasted_iota(jnp.int32, (1, RING * plane), 1)
    expert = lax.broadcasted_iota(jnp.int32, (experts_total, RING * plane), 0)
    keep = (
        lax.broadcasted_iota(jnp.int32, (SLOTS, RING * plane), 1) & (SLOTS - 1)
    ) == lax.broadcasted_iota(jnp.int32, (SLOTS, RING * plane), 0)
    for color, (first, second, third) in enumerate(ORDERS):
        digit = {
            first: (slot >> 8) & (RING - 1),
            second: (slot >> 6) & (RING - 1),
            third: (slot >> 4) & (RING - 1),
        }
        expert_of = (digit["z"] << 5) + (digit["x"] << 3) + (digit["y"] << 1)
        expert_of = expert_of + ((slot >> 3) & (CORES - 1))
        spread = jnp.where(expert_of == expert, 1.0, 0.0).astype(bf16)
        for kind, values in enumerate(listed):
            wide = jnp.dot(values, spread, preferred_element_type=f32)
            row = jnp.sum(jnp.where(keep, wide, 0.0), axis=0, keepdims=True)
            for a in range(RING):
                tables[color, a, kind : kind + 1, :] = row[:, a * plane : (a + 1) * plane]
    for d in FAR_FIRST:
        for color, (first, _, _) in enumerate(ORDERS):
            send(
                tables.at[color, (at[first] + d) % RING], seen_tab.at[d - 1, color],
                tab_s, tab_r.at[d - 1], device(**{first: d}),
            )

    for load in loads[6:8]:
        load.wait()
    total_channels = blocks * channels

    pair = CORES * channels
    token_rows[tp] = conv[tp]
    squares = jnp.zeros((row_count, 1), f32)
    for g in (0,) + NEAR_FIRST:
        drain(token_rows.at[pl.ds(0, CORES if g else 1)], mix_r.at[g])
        source = (at["y"] - g + RING) % RING
        values = token_rows[pl.ds(source * CORES, CORES)].reshape(pair, row_count)
        values = jnp.transpose(values.astype(f32))
        squares = squares + jnp.sum(values * values, axis=1, keepdims=True)
        step = pair // 128
        gain = jnp.concatenate([mix_gain[pl.ds(source * step + n, 1), :] for n in range(step)], axis=1)
        product = jnp.dot(
            (values * gain).astype(bf16), v_proj[source], preferred_element_type=f32
        )
        if g == 0:
            base[...] = product
        else:
            base[...] += product
    for load in loads[8:10]:
        load.wait()
    inverse = lax.rsqrt(squares / total_channels + EPS)
    stream = v_residual[...].astype(f32) + base[...] * inverse
    base[...] = stream
    norm = lax.rsqrt(jnp.mean(stream * stream, axis=1, keepdims=True) + EPS)
    normed[...] = (stream * norm * ffn_gain[...]).astype(bf16)

    def lead(color, i, d):
        return (d, i) if color == 2 else (i, d)

    def piece(ref, lane_at, g, h):
        color, c0, w = LANES[lane_at]
        cols = pl.ds(c0, w)
        if color == 0:
            return ref.at[:, :, g, h, :, cols]
        if color == 1:
            return ref.at[g, :, :, h, :, cols]
        return ref.at[:, g, :, h, :, cols]

    def gather_send(q, d, src, s):
        color = LANES[q][0]
        step = 1 if d == 1 or (d == 2 and q % 2 == 0) else -1
        send(src, ag[q].at[d - 1], s, ag_r.at[q, d - 1], device(**{ORDERS[color][0]: step}))

    for d in (1, 3):
        for q, (_, c0, w) in enumerate(LANES):
            gather_send(q, d, normed.at[:, pl.ds(c0, w)], ag_s.at[d - 1])

    numbers = (lax.broadcasted_iota(jnp.int32, (row_count, plane), 0) + 1).astype(f32)

    def table(color, i):
        return tables[color, at[ORDERS[color][0]]] if i == 0 else seen_tab[i - 1, color]

    def pick_rows(q, i):
        color, c0, w = LANES[q]
        second = ORDERS[color][1]
        if i == 0:
            rows = normed[:, c0 : c0 + w]
        else:
            drain(ag[q].at[i - 1], ag_r.at[q, i - 1])
            if i == (3 if q % 2 else 1):
                gather_send(q, 2, ag[q].at[i - 1], ag_s.at[1])
            rows = ag[q][i - 1]
        onehot = jnp.where(numbers == table(color, i)[0:1, :], 1.0, 0.0).astype(bf16)
        picked = lax.dot_general(
            onehot, rows, (((0,), (0,)), ((), ())), preferred_element_type=f32
        )
        picked = picked.astype(bf16).reshape(RING, RING * CORES, SLOTS, w)
        for b in range(RING):
            pick[q][b, i] = picked[b]
        for d in FAR_FIRST:
            send(
                pick[q].at[(at[second] + d) % RING, i], mid[q].at[lead(color, i, d)],
                p2_s, p2_r.at[q], device(**{second: d}),
            )
        mid[q][lead(color, i, 0)] = pick[q][at[second], i]

    def swish(gate_part, up_part):
        return (gate_part / (1.0 + jnp.exp(-gate_part)) * up_part).astype(bf16)

    for q in range(lanes):
        pick_rows(q, 0)
    for load in loads[10:13]:
        load.wait()
    rows = normed[...]
    shared = swish(
        jnp.dot(rows, v_sgate[...], preferred_element_type=f32),
        jnp.dot(rows, v_sup[...], preferred_element_type=f32),
    )
    base[...] += jnp.dot(shared, v_sdown[...], preferred_element_type=f32)
    for i in NEAR_FIRST:
        drain(seen_tab.at[i - 1], tab_r.at[i - 1])
    for turn in ((1, 3), (3, 1), (2, 2)):
        for q in range(lanes):
            pick_rows(q, turn[q % 2])

    near, pairs = RING - 1, len(PAIRS)
    eighth = arrived.shape[-1] // (RING * CORES)

    def share(quarters=0, eighths=0):
        return arrived.at[:, :, :, :, :, pl.ds(0, (quarters * CORES + eighths) * eighth)]

    for q, (color, c0, w) in enumerate(LANES):
        third = ORDERS[color][2]
        drain(mid[q].at[pl.ds(0, near)], p2_r.at[q])
        if q == lanes - COLORS:
            drain(share(near), p2_s)
        for g, h in PAIRS:
            k = (at[third] + g) % RING * CORES + (core + h) % CORES
            send(
                mid[q].at[:, :, k], piece(arrived, q, g, h),
                p3_s, p3_r.at[q], device(h, **{third: g}),
            )
        piece(arrived, q, 0, 0)[...] = mid[q][:, :, at[third] * CORES + core]

    for load in loads[13:]:
        load.wait()
    width = arrived.shape[-1]
    block = RING * RING * CORES * SLOTS
    spans = tuple(zip((0,) + CHUNK_ENDS, CHUNK_ENDS))
    for chunk, (start, stop) in enumerate(spans):
        for q in range(chunk * COLORS, (chunk + 1) * COLORS):
            drain(mid[q].at[:, :, pl.ds(0, pairs)], p3_r.at[q])

        @pl.loop(0, RING)
        def _(zi):
            rows = arrived[zi, :, :, :, :, start:stop].reshape(block, stop - start)
            gate_part = jnp.dot(rows, v_gate[start:stop, :], preferred_element_type=f32)
            up_part = jnp.dot(rows, v_up[start:stop, :], preferred_element_type=f32)
            if chunk > 0:
                gate_part = gate_part + acc_gate[zi]
                up_part = up_part + acc_up[zi]
            if chunk + 1 == len(spans):
                hidden[zi] = swish(gate_part, up_part)
            else:
                acc_gate[zi] = gate_part
                acc_up[zi] = up_part

    for chunk, (start, stop) in enumerate(spans):

        @pl.loop(0, RING)
        def _(zi):
            done = jnp.dot(hidden[zi], v_down[:, start:stop], preferred_element_type=f32)
            result[zi, :, :, :, :, start:stop] = done.astype(bf16).reshape(
                RING, RING, CORES, SLOTS, stop - start
            )

        for color in range(COLORS):
            q = chunk * COLORS + color
            third = ORDERS[color][2]
            for g, h in PAIRS:
                send(
                    piece(result, q, g, h), back[q].at[:, :, at[third] * CORES + core],
                    r1_s, r1_r.at[q], device(-h, **{third: -g}),
                )

    for q, (color, c0, w) in enumerate(LANES):
        _, second, third = ORDERS[color]
        back[q][:, :, at[third] * CORES + core] = piece(result, q, 0, 0)[...]
        drain(back[q].at[:, :, pl.ds(0, pairs)], r1_r.at[q])
        for d in FAR_FIRST:
            src = back[q].at[d] if color == 2 else back[q].at[:, d]
            send(
                src, slots[q].at[:, at[second]], r2_s, r2_r.at[q], device(**{second: -d})
            )
        slots[q][:, at[second]] = back[q][0] if color == 2 else back[q][:, 0]
    for q, (color, c0, w) in enumerate(LANES):
        first = ORDERS[color][0]
        drain(slots[q].at[:, pl.ds(0, near)], r2_r.at[q])
        for i in FAR_FIRST + (0,):
            rows = slots[q][i].reshape(plane, w)
            tab = table(color, i)
            hit = numbers == tab[0:1, :]
            high = jnp.where(hit, tab[1:2, :], 0.0).astype(bf16)
            low = jnp.where(hit, tab[2:3, :], 0.0).astype(bf16)
            some = jnp.dot(high, rows, preferred_element_type=f32) + jnp.dot(
                low, rows, preferred_element_type=f32
            )
            if i == 0:
                own_part[:, c0 : c0 + w] = some
            else:
                part[q][i - 1] = some.astype(bf16)
                send(
                    part[q].at[i - 1], got[q].at[i - 1], r3_s, r3_r.at[q],
                    device(**{first: -i}),
                )
    for q, (_, c0, w) in enumerate(LANES):
        some = own_part[:, c0 : c0 + w] + base[:, c0 : c0 + w]
        drain(got[q], r3_r.at[q])
        for i in range(near):
            some = some + got[q][i].astype(f32)
        v_out[:, c0 : c0 + w] = some.astype(bf16)
        cols = pl.ds(c0, w)
        pltpu.make_async_copy(v_out.at[:, cols], out.at[:, cols], out_s).start()
    drain(conv.at[pl.ds(0, pairs)], mix_s)
    drain(seen_tab, tab_s)
    for n in range(near):
        drain(normed, ag_s.at[n])
    drain(share(eighths=pairs), p3_s)
    drain(share(eighths=pairs), r1_s)
    drain(share(near), r2_s)
    drain(arrived.at[pl.ds(0, near), pl.ds(0, 2)], r3_s)
    drain(v_out, out_s)


def body(
    out_gate, in_gate, conv_values, conv_taps, mix_gain, out_proj, residual, ffn_gain,
    routes, route_weights, shared_gate, shared_up, shared_down,
    expert_gate, expert_up, expert_down,
):
    length, channels = conv_values.shape
    row_count, width = residual.shape
    blocks = length // row_count
    unit = expert_gate.shape[2]
    shared_unit = shared_gate.shape[1]
    bf16, f32 = jnp.bfloat16, jnp.float32
    lanes = len(LANES)
    widths = [w for _, _, w in LANES]

    def per_lane(*shape):
        return [pltpu.VMEM(shape + (w,), bf16) for w in widths]

    def vmem(*shape, dtype=bf16):
        return pltpu.VMEM(shape, dtype)

    dma = pltpu.SemaphoreType.DMA
    near, pairs = RING - 1, len(PAIRS)
    plane = RING * RING * CORES * SLOTS
    mix_gain, ffn_gain = mix_gain.reshape(-1, 128), ffn_gain.reshape(1, width)
    routes, route_weights = routes.T, route_weights.T
    small = (conv_taps, mix_gain, ffn_gain, routes, route_weights)
    scratch = (
        [vmem(row_count, width)]
        + [vmem(*a.shape, dtype=a.dtype) for a in small]
        + [vmem(channels, length)] * 3
        + [vmem(RING, CORES * channels, width), vmem(row_count, width)]
        + [vmem(width, shared_unit), vmem(width, shared_unit), vmem(shared_unit, width)]
        + [vmem(width, unit), vmem(width, unit), vmem(unit, width)]
        + [vmem(channels, row_count + length, dtype=f32), vmem(8, 2 * row_count, dtype=f32)]
        + [vmem(8, 2 * row_count, dtype=f32)]
        + [vmem(blocks, channels, row_count)] * 2
        + [vmem(row_count, width, dtype=f32), vmem(row_count, width)]
        + [vmem(COLORS, RING, 8, plane, dtype=f32), vmem(near, COLORS, 8, plane, dtype=f32)]
        + [vmem(RING, RING, RING, CORES, SLOTS, width)] * 2
        + [vmem(RING, plane, unit, dtype=f32)] * 2
        + [vmem(RING, plane, unit), vmem(row_count, width, dtype=f32)]
        + per_lane(near, row_count)
        + per_lane(RING, RING, RING * CORES, SLOTS)
        + per_lane(RING, RING, RING * CORES, SLOTS)
        + per_lane(RING, RING, RING * CORES, SLOTS)
        + per_lane(near, row_count)
        + per_lane(near, row_count)
        + [dma((16,)), dma, dma, dma, dma((RING,)), dma, dma((near,)), dma((near,))]
        + [dma((lanes, near))]
        + [dma, dma((lanes,))] * 5
        + [dma]
    )
    hbm = pl.BlockSpec(memory_space=pl.ANY)
    return pl.pallas_call(
        layer_kernel,
        out_shape=jax.ShapeDtypeStruct((row_count, width), bf16),
        in_specs=[hbm] * 16,
        out_specs=hbm,
        scratch_shapes=scratch,
        compiler_params=pltpu.CompilerParams(
            collective_id=0, has_side_effects=True, vmem_limit_bytes=67043328
        ),
        name="whole_layer",
    )(
        out_gate.T, in_gate.T, conv_values.T, conv_taps, mix_gain,
        out_proj.reshape(RING, CORES * channels, width), residual, ffn_gain,
        routes, route_weights, shared_gate, shared_up, shared_down,
        expert_gate[0], expert_up[0], expert_down[0],
    )


def solution(mesh):
    in_specs = (
        P("sp", "tp"),
        P("sp", "tp"),
        P("sp", "tp"),
        P(None, "tp"),
        P(),
        P(),
        P(("sp", "tp"), None),
        P(),
        P(("sp", "tp"), None),
        P(("sp", "tp"), None),
        P(),
        P(),
        P(),
        P(("sp", "tp"), None, None),
        P(("sp", "tp"), None, None),
        P(("sp", "tp"), None, None),
    )
    out_specs = P(("sp", "tp"), None)
    return jax.shard_map(body, mesh=mesh, in_specs=in_specs, out_specs=out_specs, check_vma=False)
```
